512 devices in a mesh: dp: 4 (over x), kv: 64 (over z, y), tp: 2 (over core).
Axes of the slice: x: 4, y: 4, z: 16, core: 2. Of those that a mesh axis runs over, the one named last changes fastest.
Arguments:
- tokens: bfloat16 [768, 2048], P('dp', ('kv', 'tp')), may hold values from -21 to 21
- state: float32 [768, 8, 128, 128], P(('dp', 'kv'), 'tp'), may hold values from -3 to 3
- mix_gain: bfloat16 [2048], P(('kv', 'tp')), may hold values from 0.099609375 to 1.8984375
- w_query: bfloat16 [2048, 1024], P('kv', 'tp'), may hold values from -0.125 to 0.125
- w_key: bfloat16 [2048, 1024], P('kv', 'tp'), may hold values from -0.125 to 0.125
- w_value: bfloat16 [2048, 1024], P('kv', 'tp'), may hold values from -0.125 to 0.125
- w_beta: bfloat16 [2048, 8], P('kv', 'tp'), may hold values from -0.125 to 0.125
- w_decay: bfloat16 [2048, 8], P('kv', 'tp'), may hold values from -0.125 to 0.125
- decay_log: float32 [8], P('tp'), may hold values from -1.5 to 1
- head_gain: bfloat16 [128], replicated, may hold values from 0.099609375 to 1.8984375
- w_out: bfloat16 [1024, 2048], P('tp', 'kv'), may hold values from -0.1875 to 0.1875
- ff_gain: bfloat16 [2048], P(('kv', 'tp')), may hold values from 0.099609375 to 1.8984375
- w_up: bfloat16 [2048, 8192], P(None, ('kv', 'tp')), may hold values from -0.125 to 0.125
- w_down: bfloat16 [8192, 2048], P(('kv', 'tp')), may hold values from -0.25 to 0.25
Outputs:
- output: bfloat16 [768, 2048], P('dp', ('kv', 'tp'))
- new_state: float32 [768, 8, 128, 128], P(('dp', 'kv'), 'tp')
The draws below stay inside these ranges and needn't reach their ends.
All inputs are finite; a program needn't handle non-finite values.
Results may differ from the reference program's by a relative error of at most 0.013.
Values may be sent and summed in bfloat16 or wider, within the bound.
A program may use at most 64 MiB of HBM per device.

```python
import jax
import jax.numpy as jnp
from jax import lax

D = 2048
HEADS = 8
HEAD_DIM = 128
FF = 8192
BATCH = 768
KEYS = 1024
N_TP = 2


def draw_tokens(key, part):
    noise_key = jax.random.fold_in(key, 23)
    columns = jnp.arange(D, dtype=jnp.float32) / D
    entries = jnp.clip(jax.random.normal(noise_key, (BATCH, D), jnp.float32), -4.0, 4.0)
    values = entries * (4.0 ** columns)[None, :] * 0.5
    return values.astype(jnp.bfloat16)


def raised(result, own_key, source, target, parts, factor):
    owner, partner = [(jnp.arange(result.shape[axis_at]) // (result.shape[axis_at] // parts)).reshape([-1 if axis == axis_at else 1 for axis in range(result.ndim)]) for axis_at in (source, target)]
    chosen = jax.random.permutation(own_key, parts)[partner]
    strong = (owner == chosen) | (owner == (partner + parts // 2) % parts)
    return jnp.where(strong, factor * result, result)


def block_levels(rng, dims, split, low, largest):
    def one(position, shards_of):
        steps = jax.random.uniform(jax.random.fold_in(jax.random.fold_in(rng, 6), position), (shards_of,), jnp.float32, low / len(split), largest / len(split))
        return jnp.repeat(jnp.exp(steps), dims[position] // shards_of).reshape((-1,) + (1,) * (len(dims) - position - 1))

    loudness = one(*split[0])
    for cut in split[1:]:
        loudness = loudness * one(*cut)
    return loudness


def gaussian(key, shape, spread, bound, pieces=(), kind=jnp.bfloat16):
    factor_of = block_levels(key, shape, pieces, -0.22, 0.18) if pieces else 1.0
    values = jax.random.normal(key, shape, jnp.float32) * spread * factor_of
    return jnp.minimum(jnp.maximum(values, -bound), bound).astype(kind)


def gaussian_with(rng, extent, deviation, limit, split, heavy, kind=jnp.bfloat16):
    result = deviation * jax.random.normal(rng, extent, jnp.float32)
    if split:
        result = result * block_levels(rng, extent, split, -0.22, 0.18)
    return jnp.clip(raised(result, jax.random.fold_in(rng, 3), *heavy), -limit, limit).astype(kind)


def setup_inputs(seed: int = 0) -> dict:
    key_of = jax.random.split(jax.random.key(seed), 15)
    tokens = draw_tokens(jax.random.fold_in(key_of[14], 71), 0)
    state = gaussian(key_of[1], (BATCH, HEADS, HEAD_DIM, HEAD_DIM), 0.5, 3.0, ((0, 256), (1, 2)), jnp.float32)
    mix_gain = jnp.clip(1.0 + 0.18 * jax.random.normal(key_of[2], (D,), jnp.float32), 0.099609375, 1.8984375).astype(jnp.bfloat16)
    w_query = gaussian(key_of[3], (D, KEYS), D ** -0.5, 0.125, ((0, 64), (1, 2)))
    w_key = gaussian(key_of[4], (D, KEYS), D ** -0.5, 0.125, ((0, 64), (1, 2)))
    w_value = gaussian(key_of[5], (D, KEYS), D ** -0.5, 0.125, ((0, 64), (1, 2)))
    w_beta = gaussian(key_of[6], (D, HEADS), D ** -0.5, 0.125, ((0, 64), (1, 2)))
    w_decay = gaussian(key_of[7], (D, HEADS), D ** -0.5, 0.125, ((0, 64), (1, 2)))
    decay_log = jnp.clip(-1.5 + 2.5 * jax.random.uniform(key_of[8], (HEADS,), jnp.float32) ** block_levels(key_of[8], (HEADS,), ((0, 2),), -0.2, 0.2), -1.5, 1.0)
    head_gain = jnp.clip(1.0 + 0.18 * jax.random.normal(key_of[9], (HEAD_DIM,), jnp.float32), 0.099609375, 1.8984375).astype(jnp.bfloat16)
    w_out = gaussian(key_of[10], (KEYS, D), KEYS ** -0.5, 0.1875, ((0, 2), (1, 64)))
    ff_gain = jnp.clip(1.0 + 0.18 * jax.random.normal(key_of[11], (D,), jnp.float32), 0.099609375, 1.8984375).astype(jnp.bfloat16)
    w_up = gaussian(key_of[12], (D, FF), D ** -0.5, 0.125, ((1, 128),))
    w_down = gaussian_with(key_of[13], (FF, D), FF ** -0.5, 0.25, ((0, 128),), (0, 1, 128, 5.5))
    return dict(tokens=tokens, state=state, mix_gain=mix_gain, w_query=w_query, w_key=w_key, w_value=w_value, w_beta=w_beta, w_decay=w_decay, decay_log=decay_log, head_gain=head_gain, w_out=w_out, ff_gain=ff_gain, w_up=w_up, w_down=w_down)


def reference(tokens, state, mix_gain, w_query, w_key, w_value, w_beta, w_decay, decay_log, head_gain, w_out, ff_gain, w_up, w_down):
    tokens_float = tokens.astype(jnp.float32)
    mean_square = lax.optimization_barrier(jnp.mean(tokens_float * tokens_float, axis=1, keepdims=True))
    scaled = (tokens_float * mix_gain.astype(jnp.float32)).astype(jnp.bfloat16)
    inverse = lax.rsqrt(mean_square + 1e-06)
    query = inverse * jnp.dot(scaled, w_query, preferred_element_type=jnp.float32)
    key_rows = inverse * jnp.dot(scaled, w_key, preferred_element_type=jnp.float32)
    value = inverse * jnp.dot(scaled, w_value, preferred_element_type=jnp.float32)
    beta = jax.nn.sigmoid(inverse * jnp.dot(scaled, w_beta, preferred_element_type=jnp.float32))
    decay = -jnp.exp(decay_log)[None, :] * jax.nn.softplus(inverse * jnp.dot(scaled, w_decay, preferred_element_type=jnp.float32))
    batch_rows = tokens.shape[0]
    query = query.reshape(batch_rows, HEADS, HEAD_DIM)
    key_rows = key_rows.reshape(batch_rows, HEADS, HEAD_DIM)
    value = value.reshape(batch_rows, HEADS, HEAD_DIM)
    qnorm = query * lax.rsqrt(lax.optimization_barrier(jnp.sum(query * query, axis=-1, keepdims=True)) + 1e-06)
    knorm = key_rows * lax.rsqrt(lax.optimization_barrier(jnp.sum(key_rows * key_rows, axis=-1, keepdims=True)) + 1e-06)
    kept = state * jnp.exp(decay)[:, :, None, None]
    predicted = lax.optimization_barrier(jnp.sum(kept * knorm[:, :, :, None], axis=2))
    new_state = kept + (beta[:, :, None] * knorm)[:, :, :, None] * (value - predicted)[:, :, None, :]
    heads = lax.optimization_barrier(jnp.sum(new_state * qnorm[:, :, :, None], axis=2)) / jnp.sqrt(jnp.float32(HEAD_DIM))
    normed = heads * lax.rsqrt(lax.optimization_barrier(jnp.mean(heads * heads, axis=-1, keepdims=True)) + 1e-06) * head_gain.astype(jnp.float32)
    normed = normed.astype(jnp.bfloat16).reshape(batch_rows, KEYS)
    half_width = KEYS // N_TP
    mixed = jnp.zeros((batch_rows, D), jnp.float32)
    for half_index in range(N_TP):
        lower = half_index * half_width
        product = jnp.dot(normed[:, lower:lower + half_width], w_out[lower:lower + half_width], preferred_element_type=jnp.float32)
        mixed = mixed + product.astype(jnp.bfloat16).astype(jnp.float32)
    resid = (tokens_float + mixed).astype(jnp.bfloat16)
    resid_float = resid.astype(jnp.float32)
    mean_square2 = lax.optimization_barrier(jnp.mean(resid_float * resid_float, axis=1, keepdims=True))
    scaled2 = (resid_float * ff_gain.astype(jnp.float32)).astype(jnp.bfloat16)
    up_rows = jnp.dot(scaled2, w_up, preferred_element_type=jnp.float32) * lax.rsqrt(mean_square2 + 1e-06)
    act = jnp.square(jax.nn.relu(up_rows)).astype(jnp.bfloat16)
    output = (resid_float + jnp.dot(act, w_down, preferred_element_type=jnp.float32)).astype(jnp.bfloat16)
    return (output, new_state)
```

```python
import functools

import jax
import jax.numpy as jnp
from jax import lax
from jax.experimental import pallas as pl
from jax.experimental.pallas import tpu as pltpu
from jax.sharding import PartitionSpec as P

D = 2048
NZ = 16
NY = 4
MESH = pl.DeviceIdType.MESH
F32 = jnp.float32
BF16 = jnp.bfloat16
NT = (((1,), (1,)), ((), ()))
R1 = 40
R3 = 32


def iota(shape, dim):
    return lax.broadcasted_iota(jnp.int32, shape, dim)


def body(
    tile_hbm,
    state_hbm,
    wq_hbm,
    wk_hbm,
    wv_hbm,
    wo_hbm,
    wu_hbm,
    wd_hbm,
    head_gain_ref,
    decay_log_ref,
    out_ref,
    state_out,
    tbuf,
    wbuf,
    wo,
    fbuf,
    st,
    qbuf,
    xs,
    zs,
    zsend,
    zrecv,
    accs,
    g12,
    hs,
    nsend,
    nrecv,
    nf,
    rsend,
    rrecv,
    res,
    dsend,
    drecv,
    ysend,
    yrecv,
    lsem,
    ssem,
    rsem,
):
    kv = lax.axis_index("kv")
    tp = lax.axis_index("tp")
    z = kv // NY
    y = kv % NY
    me8 = y * 2 + tp
    half = z // 8

    barrier = pltpu.get_barrier_semaphore()

    def greet_z(j, carry):
        t = (z * 2 + tp + j) % (2 * NZ)
        pl.semaphore_signal(
            barrier, inc=1, device_id={"kv": (t // 2) * NY + y, "tp": t % 2}, device_id_type=MESH
        )
        return carry

    lax.fori_loop(1, 2 * NZ, greet_z, 0)

    def greet_y(j, carry):
        other = z * NY + (y + j) % NY
        for t in range(2):
            pl.semaphore_signal(
                barrier, inc=1, device_id={"kv": other, "tp": t}, device_id_type=MESH
            )
        return carry

    lax.fori_loop(1, NY, greet_y, 0)

    def local(src, dst, k):
        return pltpu.make_async_copy(src, dst, lsem.at[k])

    loads = [
        local(tile_hbm, tbuf.at[me8], 0),
        local(wq_hbm, wbuf.at[y, 0], 1),
        local(wk_hbm, wbuf.at[y, 1], 2),
        local(wv_hbm, wbuf.at[y, 2], 3),
        local(
            wo_hbm,
            wo.at[pl.ds(pl.multiple_of(y * 32, 32), 32), pl.ds(pl.multiple_of(tp * 512, 512), 512)],
            4,
        ),
        local(wu_hbm, fbuf.at[tp, y, 0], 5),
        local(wd_hbm, fbuf.at[tp, y, 1], 6),
        local(state_hbm, st, 7),
    ]
    for c in loads:
        c.start()

    src_row, seq_col = iota((1024, 256), 0), iota((1024, 256), 1)
    lane = src_row % 128
    place = 12 * ((src_row // 128 % 2) * 8 + lane % 8) + 3 * (src_row // 256) + lane // 8
    qbuf[...] = jnp.where((seq_col == place) & (lane < 24), 1.0, 0.0).astype(BF16)

    row, col = iota((56, 256), 0), iota((56, 256), 1)
    wanted = jnp.where(row < 48, 12 * (row % 16) + 3 * y + row // 16, row + 144)
    pick = jnp.where((col == wanted) & (row < 50), 1.0, 0.0).astype(BF16)

    er, ec = iota((512, 128), 0), iota((512, 128), 1)
    spread = jnp.where((ec == er // 128 * 32 + er % 128) & (er % 128 < 32), 1.0, 0.0).astype(BF16)

    for c in loads[:7]:
        c.wait()

    pl.semaphore_wait(barrier, 2 * NZ - 1 + 2 * (NY - 1))

    def push(src, dst, k, where):
        pltpu.make_async_remote_copy(
            src_ref=src,
            dst_ref=dst,
            send_sem=ssem.at[k],
            recv_sem=rsem.at[k],
            device_id=where,
            device_id_type=MESH,
        ).start()

    def to_eight(src_of, dst, k):
        def one(j, carry):
            p = (me8 + j) % 8
            push(src_of(p), dst, k, {"kv": z * NY + p // 2, "tp": p % 2})
            return carry

        lax.fori_loop(1, 8, one, 0)

    def to_column(ref, k):
        def one(j, carry):
            push(ref, ref, k, {"kv": z * NY + (y + j) % NY})
            return carry

        lax.fori_loop(1, NY, one, 0)

    def got(ref, sem):
        pltpu.make_async_copy(ref, ref, sem).wait()

    my_wo = wo.at[
        pl.ds(pl.multiple_of(y * 32, 32), 32), pl.ds(pl.multiple_of(tp * 512, 512), 512)
    ]
    to_eight(lambda p: tbuf.at[me8], tbuf.at[me8], 0)
    to_column(wbuf.at[y], 1)
    to_eight(lambda p: my_wo, my_wo, 2)
    to_column(fbuf.at[tp, y], 3)

    got(tbuf.at[pl.ds(0, 7)], rsem.at[0])
    tiles = tbuf[...]
    turned = tiles[:, :16, :].reshape(128, 256)
    chosen = lax.dot_general(pick, turned, NT, preferred_element_type=F32)
    xs[...] = chosen
    x = chosen[:48]
    scaled = (x * chosen[48:49]).astype(BF16)
    square = jnp.sum(x * x, axis=1, keepdims=True)
    square_hi = square.astype(BF16).astype(F32)
    own = jnp.concatenate([tbuf[2 * k + tp, 16:32, :128] for k in range(NY)], axis=1)
    gate_w = jnp.dot(own, spread, preferred_element_type=F32).astype(BF16)
    gate_w = jnp.concatenate([gate_w, jnp.zeros((112, 128), BF16)], axis=0)
    gate = lax.dot_general(scaled, gate_w, NT, preferred_element_type=F32)
    gl = iota((48, 128), 1)
    gate = jnp.where(gl == 8, square_hi, jnp.where(gl == 9, square - square_hi, gate))

    got(wbuf.at[pl.ds(0, 3)], rsem.at[1])
    for m in range(3):
        weight = wbuf[:, m].reshape(128, 512)
        part = jnp.dot(scaled, weight, preferred_element_type=F32)
        for h in range(4):
            for i in range(3):
                zs[pl.ds(m * 12 + h * 3 + i, NZ, R1), :] = part[
                    i * 16 : (i + 1) * 16, h * 128 : (h + 1) * 128
                ]
    for i in range(3):
        zs[pl.ds(36 + i, NZ, R1), :] = gate[i * 16 : (i + 1) * 16]
    zs[pl.ds(39, NZ, R1), :] = jnp.zeros((NZ, 128), F32)
    zsend[...] = zs[...].reshape(NZ, R1, 128).astype(BF16)

    def along(src_of, dst, k):
        def one(n, carry):
            d = NZ // 2 + ((n + 1) // 2) * (1 - 2 * (n % 2))
            far = (z + d) % NZ
            push(src_of(far), dst, k, {"kv": far * NY + y})
            return carry

        lax.fori_loop(0, NZ - 1, one, 0)

    along(lambda far: zsend.at[far], zrecv.at[z], 4)
    zrecv[z] = zsend[z]
    loads[7].wait()
    got(zrecv.at[pl.ds(0, NZ - 1)], rsem.at[4])

    acc = zrecv[0].astype(F32)
    for k in range(1, NZ):
        acc = acc + zrecv[k].astype(F32)
    accs[...] = acc
    for h in range(4):
        g12[3 * h : 3 * h + 3, :] = accs[36:39, :]
    g = g12[0:12, :]
    r12, l12 = iota((12, 128), 0), iota((12, 128), 1)
    head_of = r12 // 3

    def take(mask):
        return jnp.sum(jnp.where(mask, g, 0.0), axis=1, keepdims=True)

    inverse = lax.rsqrt(take((l12 == 8) | (l12 == 9)) / D + 1e-06)
    beta = jax.nn.sigmoid(inverse * take(l12 == head_of))
    u = inverse * take(l12 == head_of + 4)
    soft = jnp.maximum(u, 0.0) + jnp.log1p(jnp.exp(-jnp.abs(u)))
    h1 = iota((12, 1), 0) // 3
    rate = jnp.where(
        h1 == 0,
        decay_log_ref[0],
        jnp.where(h1 == 1, decay_log_ref[1], jnp.where(h1 == 2, decay_log_ref[2], decay_log_ref[3])),
    )
    keep = jnp.exp(-jnp.exp(rate) * soft)
    query = inverse * accs[0:12, :]
    key = inverse * accs[12:24, :]
    value = inverse * accs[24:36, :]
    qnorm = query * lax.rsqrt(jnp.sum(query * query, axis=1, keepdims=True) + 1e-06)
    knorm = key * lax.rsqrt(jnp.sum(key * key, axis=1, keepdims=True) + 1e-06)
    pad = jnp.zeros((104, 128), F32)
    g12[0:12, :] = qnorm
    g12[12:24, :] = knorm
    both = jnp.concatenate([g12[...], pad], axis=0).T
    for r in range(12):
        h, i = r // 3, r % 3
        kc = both[:, 12 + r : 13 + r]
        qc = both[:, r : r + 1]
        kept = st[i, h] * keep[r : r + 1, :]
        predicted = jnp.sum(kept * kc, axis=0, keepdims=True)
        new = kept + kc * (beta[r : r + 1, :] * (value[r : r + 1, :] - predicted))
        st[i, h] = new
        hs[r : r + 1, :] = jnp.sum(new * qc, axis=0, keepdims=True)
    heads = hs[...] / jnp.sqrt(jnp.float32(128))
    heads = jnp.where(iota((16, 128), 0) < 12, heads, 0.0)
    normed = (
        heads
        * lax.rsqrt(jnp.mean(heads * heads, axis=1, keepdims=True) + 1e-06)
        * head_gain_ref[...].astype(F32)
    )
    nsend[...] = normed.astype(BF16)
    state_copy = local(st, state_out, 8)
    state_copy.start()

    slot = (z % 8) * 2 + tp

    def spread_heads(n, carry):
        d = (NZ // 2 + ((n + 1) // 2) * (1 - 2 * (n % 2))) % NZ
        far = (z + d) % NZ
        push(nsend, nrecv.at[slot], 5, {"kv": far * NY + y, "tp": half})
        return carry

    lax.fori_loop(0, NZ - 1, spread_heads, 0)

    @pl.when(half == tp)
    def _():
        nrecv[slot] = nsend[...]
        got(nrecv.at[pl.ds(0, 15)], rsem.at[5])

    @pl.when(half != tp)
    def _():
        push(nsend, nrecv.at[slot], 5, {"tp": half})
        got(nrecv, rsem.at[5])

    got(wo.at[pl.ds(0, 112), :], rsem.at[2])
    nf[...] = nrecv[...].astype(F32).reshape(256, 128)
    wide = jnp.concatenate(
        [
            jnp.concatenate(
                [nf[pl.ds(t * 16 + h * 3 + i, 8, 32), :] for i in range(3)], axis=0
            )
            for t in range(2)
            for h in range(4)
        ],
        axis=1,
    ).astype(BF16)
    mixed = lax.dot_general(wide, wo[...], NT, preferred_element_type=F32)
    mine = jnp.concatenate(
        [xs[pl.ds(pl.multiple_of(i * 16 + tp * 8, 8), 8), :] for i in range(3)], axis=0
    )
    resid = (mine + mixed).astype(BF16).astype(F32)
    res[...] = resid
    scaled2 = (resid * xs[49:50, :]).astype(BF16).astype(F32)
    total = lax.dot_general(
        jnp.ones((8, 128), F32),
        jnp.concatenate([resid * resid, jnp.zeros((104, 128), F32)], axis=0),
        NT,
        preferred_element_type=F32,
        precision=lax.Precision.HIGHEST,
    )
    total_hi = total.astype(BF16).astype(F32)
    r8 = iota((8, 128), 0)
    tail = jnp.where(r8 == 0, total_hi, jnp.where(r8 == 1, total - total_hi, 0.0))
    rsend[...] = jnp.concatenate([scaled2, tail], axis=0).astype(BF16)
    along(lambda far: rsend, rrecv.at[z], 6)
    rrecv[z] = rsend[...]
    got(fbuf.at[tp, pl.ds(0, 3)], rsem.at[3])
    push(fbuf.at[tp], fbuf.at[tp], 7, {"tp": 1 - tp})
    got(rrecv.at[pl.ds(0, NZ - 1)], rsem.at[6])
    rows = jnp.concatenate([rrecv[k] for k in range(NZ)], axis=1)
    sums = rrecv[0, 16:32, :].astype(F32)
    for k in range(1, NZ):
        sums = sums + rrecv[k, 16:32, :].astype(F32)
    squares = sums[8:9] + sums[9:10]
    scale = lax.rsqrt(squares / D + 1e-06)
    dr, dc = iota((R3, 128), 0), iota((R3, 128), 1)
    scale = jnp.sum(jnp.where(dr == dc, scale, 0.0), axis=1, keepdims=True)
    got(fbuf.at[0], rsem.at[7])
    up_w = fbuf[:, :, 0].reshape(512, D)
    up = lax.dot_general(rows, up_w, NT, preferred_element_type=F32) * scale
    act = jnp.square(jnp.maximum(up, 0.0)).astype(BF16)
    for k in range(NZ // 2):
        part = jnp.dot(
            act,
            fbuf[:, :, 1, :, k * 256 : (k + 1) * 256].reshape(512, 256),
            preferred_element_type=F32,
        ).astype(BF16)
        dsend[2 * k] = part[:24, :128]
        dsend[2 * k + 1] = part[:24, 128:]
    along(lambda far: dsend.at[far], drecv.at[z], 8)
    drecv[z] = dsend[z]
    got(drecv.at[pl.ds(0, NZ - 1)], rsem.at[8])
    final = res[...]
    for k in range(NZ):
        final = final + drecv[k].astype(F32)
    final = jnp.concatenate([final, jnp.zeros((104, 128), F32)], axis=0).T
    ysend[...] = final.astype(BF16).reshape(8, 16, 128)
    to_eight(lambda p: ysend.at[p], yrecv.at[me8], 9)
    yrecv[me8] = ysend[me8]
    got(yrecv.at[pl.ds(0, 7)], rsem.at[9])
    pieces = jnp.concatenate([yrecv[k] for k in range(8)], axis=1)
    placed = jnp.dot(pieces, qbuf[...], preferred_element_type=F32)
    out_ref[...] = placed[:, :192].astype(BF16)

    state_copy.wait()
    got(tbuf.at[pl.ds(0, 7)], ssem.at[0])
    got(wbuf.at[pl.ds(0, 3)], ssem.at[1])
    got(wo.at[pl.ds(0, 112), :], ssem.at[2])
    got(fbuf.at[tp, pl.ds(0, 3)], ssem.at[3])
    got(zsend.at[pl.ds(0, NZ - 1)], ssem.at[4])

    @pl.when(half == tp)
    def _():
        got(nrecv.at[pl.ds(0, 15)], ssem.at[5])

    @pl.when(half != tp)
    def _():
        got(nrecv, ssem.at[5])

    got(rrecv.at[pl.ds(0, NZ - 1)], ssem.at[6])
    got(fbuf.at[tp], ssem.at[7])
    got(dsend.at[pl.ds(0, NZ - 1)], ssem.at[8])
    got(ysend.at[pl.ds(0, 7)], ssem.at[9])


def local_step(
    tokens,
    state,
    mix_gain,
    w_query,
    w_key,
    w_value,
    w_beta,
    w_decay,
    decay_log,
    head_gain,
    w_out,
    ff_gain,
    w_up,
    w_down,
):
    upper = jnp.concatenate(
        [tokens.T, mix_gain[:, None], ff_gain[:, None], jnp.zeros((16, 62), BF16)], axis=1
    )
    lower = jnp.concatenate([w_beta.T, w_decay.T], axis=0)
    tile = jnp.concatenate([upper, jnp.pad(lower, ((0, 8), (0, 224)))], axis=0)
    anywhere = pl.BlockSpec(memory_space=pltpu.HBM)
    vmem = pl.BlockSpec(memory_space=pltpu.VMEM)
    out, new_state = pl.pallas_call(
        body,
        name="layer",
        out_shape=(
            jax.ShapeDtypeStruct((16, 192), BF16),
            jax.ShapeDtypeStruct(state.shape, F32),
        ),
        in_specs=[anywhere] * 8 + [vmem, pl.BlockSpec(memory_space=pltpu.SMEM)],
        out_specs=(vmem, anywhere),
        scratch_shapes=[
            pltpu.VMEM((8, 32, 256), BF16),
            pltpu.VMEM((NY, 3, 32, 512), BF16),
            pltpu.VMEM((128, 1024), BF16),
            pltpu.VMEM((2, NY, 2, 64, D), BF16),
            pltpu.VMEM((3, 4, 128, 128), F32),
            pltpu.VMEM((1024, 256), BF16),
            pltpu.VMEM((56, 128), F32),
            pltpu.VMEM((NZ * R1, 128), F32),
            pltpu.VMEM((NZ, R1, 128), BF16),
            pltpu.VMEM((NZ, R1, 128), BF16),
            pltpu.VMEM((R1, 128), F32),
            pltpu.VMEM((24, 128), F32),
            pltpu.VMEM((16, 128), F32),
            pltpu.VMEM((16, 128), BF16),
            pltpu.VMEM((16, 16, 128), BF16),
            pltpu.VMEM((256, 128), F32),
            pltpu.VMEM((R3, 128), BF16),
            pltpu.VMEM((NZ, R3, 128), BF16),
            pltpu.VMEM((24, 128), F32),
            pltpu.VMEM((NZ, 24, 128), BF16),
            pltpu.VMEM((NZ, 24, 128), BF16),
            pltpu.VMEM((8, 16, 128), BF16),
            pltpu.VMEM((8, 16, 128), BF16),
            pltpu.SemaphoreType.DMA((9,)),
            pltpu.SemaphoreType.DMA((10,)),
            pltpu.SemaphoreType.DMA((10,)),
        ],
        compiler_params=pltpu.CompilerParams(
            collective_id=0, has_side_effects=True, vmem_limit_bytes=32 * 1024 * 1024
        ),
    )(
        tile,
        state,
        w_query,
        w_key,
        w_value,
        w_out.T,
        w_up.T,
        w_down,
        head_gain[None, :],
        decay_log,
    )
    return out.T, new_state


def solution(mesh):
    placed = (
        P("dp", ("kv", "tp")),
        P(("dp", "kv"), "tp", None, None),
        P(("kv", "tp")),
        P("kv", "tp"),
        P("kv", "tp"),
        P("kv", "tp"),
        P("kv", "tp"),
        P("kv", "tp"),
        P("tp"),
        P(),
        P("tp", "kv"),
        P(("kv", "tp")),
        P(None, ("kv", "tp")),
        P(("kv", "tp"), None),
    )
    return jax.shard_map(
        local_step,
        mesh=mesh,
        in_specs=placed,
        out_specs=(P("dp", ("kv", "tp")), P(("dp", "kv"), "tp", None, None)),
        check_vma=False,
    )
```

```python
import functools

import jax
import jax.numpy as jnp
from jax import lax
from jax.experimental import pallas as pl
from jax.experimental.pallas import tpu as pltpu
from jax.sharding import PartitionSpec as P

D = 2048
NZ = 16
NY = 4
MESH = pl.DeviceIdType.MESH
F32 = jnp.float32
BF16 = jnp.bfloat16
NT = (((1,), (1,)), ((), ()))
R1 = 40
GATE_AT = 200
R3 = 32


def iota(shape, dim):
    return lax.broadcasted_iota(jnp.int32, shape, dim)


def body(
    tokens_hbm,
    mix_gain_hbm,
    ff_gain_hbm,
    beta_hbm,
    decay_hbm,
    head_gain_hbm,
    decay_log_hbm,
    state_hbm,
    wq_hbm,
    wk_hbm,
    wv_hbm,
    wo_hbm,
    wu_hbm,
    wd_hbm,
    out_ref,
    vec_ref,
    tok,
    mixg,
    ffg,
    bta,
    dcy,
    hgain,
    dlog,
    tbuf,
    wbuf,
    wo,
    fbuf,
    st,
    qbuf,
    ebuf,
    xs,
    zs,
    zsend,
    zrecv,
    accs,
    g12,
    hs,
    nsend,
    nrecv,
    nf,
    rsend,
    rrecv,
    res,
    dsend,
    drecv,
    ysend,
    yrecv,
    lsem,
    ssem,
    rsem,
    fsem,
    near_sem,
    mid_sem,
    far_sem,
):
    kv = lax.axis_index("kv")
    tp = lax.axis_index("tp")
    z = kv // NY
    y = kv % NY
    me8 = y * 2 + tp
    half = z // 8

    barrier = pltpu.get_barrier_semaphore()

    def greet(sem, where):
        pl.semaphore_signal(sem, inc=1, device_id=where, device_id_type=MESH)

    def on_ring(d):
        return {"kv": ((z + d) % NZ) * NY + y}

    def greet_eight(j, carry):
        p = (me8 + j) % 8
        greet(barrier, {"kv": z * NY + p // 2, "tp": p % 2})
        return carry

    lax.fori_loop(1, 8, greet_eight, 0)
    greet(barrier, on_ring(1))
    greet(barrier, on_ring(NZ - 1))

    def local(src, dst, k):
        return pltpu.make_async_copy(src, dst, lsem.at[k])

    my_wo = wo.at[
        pl.ds(pl.multiple_of(y * 32, 32), 32), pl.ds(pl.multiple_of(tp * 512, 512), 512)
    ]
    loads = [
        local(tokens_hbm, tok, 0),
        local(mix_gain_hbm, mixg, 1),
        local(ff_gain_hbm, ffg, 2),
        local(beta_hbm, bta, 3),
        local(decay_hbm, dcy, 4),
        local(wq_hbm, wbuf.at[y, 0], 5),
        local(wk_hbm, wbuf.at[y, 1], 6),
        local(wv_hbm, wbuf.at[y, 2], 7),
        local(wo_hbm, my_wo, 8),
        local(wu_hbm, fbuf.at[tp, y, 0], 9),
        local(wd_hbm, fbuf.at[tp, y, 1], 10),
        local(head_gain_hbm, hgain, 11),
        local(decay_log_hbm, dlog, 12),
        local(state_hbm, st, 13),
    ]
    for c in loads:
        c.start()

    src_row, seq_col = iota((1024, 256), 0), iota((1024, 256), 1)
    lane = src_row % 128
    place = 12 * ((src_row // 128 % 2) * 8 + lane % 8) + 3 * (src_row // 256) + lane // 8
    qbuf[...] = jnp.where((seq_col == place) & (lane < 24), 1.0, 0.0).astype(BF16)

    row, col = iota((56, 256), 0), iota((56, 256), 1)
    wanted = jnp.where(row < 48, 12 * (row % 16) + 3 * y + row // 16, row + 144)
    pick = jnp.where((col == wanted) & (row < 50), 1.0, 0.0).astype(BF16)

    er, ec = iota((1024, 128), 0), iota((1024, 128), 1)
    into = er % 256 - GATE_AT
    spread = jnp.where((ec == er // 256 * 32 + into) & (into >= 0) & (into < 32), 1.0, 0.0)
    ebuf[...] = spread.astype(BF16)
    pr, pc = iota((32, 256), 0), iota((32, 256), 1)
    shift = jnp.where(pc == pr + GATE_AT, 1.0, 0.0).astype(BF16)

    for c in loads[:5]:
        c.wait()
    sr, sc = iota((16, 16), 0), iota((16, 16), 1)

    def upright(ref):
        return jnp.sum(jnp.where(sr == sc, ref[...].astype(F32), 0.0), axis=1, keepdims=True)

    gate_rows = jnp.concatenate([bta[...].astype(F32), dcy[...].astype(F32)], axis=0)
    gate_rows = jnp.concatenate([gate_rows, jnp.zeros((8, 32), F32)], axis=0).astype(BF16)
    lanes = iota((16, 256), 1)
    tile = jnp.dot(gate_rows, shift, preferred_element_type=F32)
    tile = jnp.where(lanes == 192, upright(mixg), jnp.where(lanes == 193, upright(ffg), tile))
    tile = tile + jnp.concatenate([tok[...].astype(F32), jnp.zeros((16, 64), F32)], axis=1)
    tbuf[me8] = tile.astype(BF16)
    for c in loads[5:11]:
        c.wait()

    pl.semaphore_wait(barrier, 9)

    def push(src, dst, k, where, to=None):
        pltpu.make_async_remote_copy(
            src_ref=src,
            dst_ref=dst,
            send_sem=ssem.at[k],
            recv_sem=rsem.at[k] if to is None else to,
            device_id=where,
            device_id_type=MESH,
        ).start()

    def to_eight(src_of, dst, k):
        def one(j, carry):
            p = (me8 + j) % 8
            push(src_of(p), dst, k, {"kv": z * NY + p // 2, "tp": p % 2})
            return carry

        lax.fori_loop(1, 8, one, 0)

    above, below, across = (y + 1) % NY, (y + NY - 1) % NY, (y + 2) % NY

    def at_y(other):
        return {"kv": z * NY + other}

    def got(ref, sem):
        pltpu.make_async_copy(ref, ref, sem).wait()

    to_eight(lambda p: tbuf.at[me8], tbuf.at[me8], 0)
    push(wbuf.at[y], wbuf.at[y], 1, at_y(above), fsem.at[0])
    push(wbuf.at[y], wbuf.at[y], 1, at_y(below), fsem.at[1])
    greet(near_sem, on_ring(1))
    greet(near_sem, on_ring(NZ - 1))
    pl.semaphore_wait(near_sem, 2)
    greet(mid_sem, on_ring(2))
    greet(mid_sem, on_ring(NZ - 2))
    pl.semaphore_wait(mid_sem, 2)
    greet(far_sem, on_ring(4))
    greet(far_sem, on_ring(NZ - 4))
    got(wbuf.at[y], fsem.at[0])
    upper_half = wbuf.at[below, :, pl.ds(0, 16)]
    push(upper_half, upper_half, 2, at_y(above), fsem.at[2])
    got(wbuf.at[y], fsem.at[1])
    lower_half = wbuf.at[above, :, pl.ds(16, 16)]
    push(lower_half, lower_half, 2, at_y(below), fsem.at[3])
    for other in (above, below, across):
        push(my_wo, my_wo, 10, at_y(other))
    push(fbuf.at[tp, y], fbuf.at[tp, y], 3, at_y(above), fsem.at[4])
    push(fbuf.at[tp, y], fbuf.at[tp, y], 3, at_y(below), fsem.at[5])
    push(fbuf.at[tp, y], fbuf.at[tp, y], 7, {"tp": 1 - tp}, fsem.at[8])

    got(tbuf.at[pl.ds(0, 7)], rsem.at[0])
    tiles = tbuf[...]
    turned = tiles.reshape(128, 256)
    chosen = lax.dot_general(pick, turned, NT, preferred_element_type=F32)
    xs[...] = chosen
    x = chosen[:48]
    scaled = (x * chosen[48:49]).astype(BF16)
    square = jnp.sum(x * x, axis=1, keepdims=True)
    square_hi = square.astype(BF16).astype(F32)
    own = jnp.concatenate([tbuf[2 * k + tp] for k in range(NY)], axis=1)
    gate_w = jnp.dot(own, ebuf[...], preferred_element_type=F32)
    gate_w = jnp.where(iota((16, 128), 0) < 8, gate_w, 0.0).astype(BF16)
    gate_w = jnp.concatenate([gate_w, jnp.zeros((112, 128), BF16)], axis=0)
    gate = lax.dot_general(scaled, gate_w, NT, preferred_element_type=F32)
    gl = iota((48, 128), 1)
    gate = jnp.where(gl == 8, square_hi, jnp.where(gl == 9, square - square_hi, gate))

    got(upper_half, fsem.at[2])
    got(lower_half, fsem.at[3])
    for m in range(3):
        weight = wbuf[:, m].reshape(128, 512)
        part = jnp.dot(scaled, weight, preferred_element_type=F32)
        for h in range(4):
            for i in range(3):
                zs[pl.ds(m * 12 + h * 3 + i, NZ, R1), :] = part[
                    i * 16 : (i + 1) * 16, h * 128 : (h + 1) * 128
                ]
    for i in range(3):
        zs[pl.ds(36 + i, NZ, R1), :] = gate[i * 16 : (i + 1) * 16]
    zs[pl.ds(39, NZ, R1), :] = jnp.zeros((NZ, 128), F32)
    zsend[...] = zs[...].reshape(NZ, R1, 128).astype(BF16)

    pl.semaphore_wait(far_sem, 2)

    def along(src_of, dst, k):
        def one(n, carry):
            d = NZ // 2 + ((n + 1) // 2) * (1 - 2 * (n % 2))
            far = (z + d) % NZ
            push(src_of(far), dst, k, {"kv": far * NY + y})
            return carry

        lax.fori_loop(0, NZ - 1, one, 0)

    along(lambda far: zsend.at[far], zrecv.at[z], 4)
    zrecv[z] = zsend[z]
    for c in loads[11:]:
        c.wait()
    got(zrecv.at[pl.ds(0, NZ - 1)], rsem.at[4])

    acc = zrecv[0].astype(F32)
    for k in range(1, NZ):
        acc = acc + zrecv[k].astype(F32)
    accs[...] = acc
    for h in range(4):
        g12[3 * h : 3 * h + 3, :] = accs[36:39, :]
    g = g12[0:12, :]
    r12, l12 = iota((12, 128), 0), iota((12, 128), 1)
    head_of = r12 // 3

    def take(mask):
        return jnp.sum(jnp.where(mask, g, 0.0), axis=1, keepdims=True)

    inverse = lax.rsqrt(take((l12 == 8) | (l12 == 9)) / D + 1e-06)
    beta = jax.nn.sigmoid(inverse * take(l12 == head_of))
    u = inverse * take(l12 == head_of + 4)
    soft = jnp.maximum(u, 0.0) + jnp.log1p(jnp.exp(-jnp.abs(u)))
    lr, lc = iota((12, 4), 0), iota((12, 4), 1)
    rate = jnp.sum(jnp.where(lc == lr // 3, dlog[...], 0.0), axis=1, keepdims=True)
    keep = jnp.exp(-jnp.exp(rate) * soft)
    query = inverse * accs[0:12, :]
    key = inverse * accs[12:24, :]
    value = inverse * accs[24:36, :]
    qnorm = query * lax.rsqrt(jnp.sum(query * query, axis=1, keepdims=True) + 1e-06)
    knorm = key * lax.rsqrt(jnp.sum(key * key, axis=1, keepdims=True) + 1e-06)
    pad = jnp.zeros((104, 128), F32)
    g12[0:12, :] = qnorm
    g12[12:24, :] = knorm
    both = jnp.concatenate([g12[...], pad], axis=0).T
    for r in range(12):
        h, i = r // 3, r % 3
        kc = both[:, 12 + r : 13 + r]
        qc = both[:, r : r + 1]
        kept = st[i, h] * keep[r : r + 1, :]
        predicted = jnp.sum(kept * kc, axis=0, keepdims=True)
        change = beta[r : r + 1, :] * (value[r : r + 1, :] - predicted)
        vec_ref[12 + r : 13 + r, :] = change
        hs[r : r + 1, :] = jnp.sum((kept + kc * change) * qc, axis=0, keepdims=True)
    vec_ref[0:12, :] = knorm
    vec_ref[24:36, :] = jnp.broadcast_to(keep, (12, 128))
    heads = hs[...] / jnp.sqrt(jnp.float32(128))
    heads = jnp.where(iota((16, 128), 0) < 12, heads, 0.0)
    normed = (
        heads
        * lax.rsqrt(jnp.mean(heads * heads, axis=1, keepdims=True) + 1e-06)
        * hgain[...].astype(F32)
    )
    nsend[...] = normed.astype(BF16)

    slot = (z % 8) * 2 + tp

    def spread_heads(n, carry):
        d = (NZ // 2 + ((n + 1) // 2) * (1 - 2 * (n % 2))) % NZ
        far = (z + d) % NZ
        push(nsend, nrecv.at[slot], 5, {"kv": far * NY + y, "tp": half})
        return carry

    lax.fori_loop(0, NZ - 1, spread_heads, 0)

    @pl.when(half == tp)
    def _():
        nrecv[slot] = nsend[...]

    @pl.when(half != tp)
    def _():
        push(nsend, nrecv.at[slot], 5, {"tp": half})

    my_lanes = wo.at[:, pl.ds(pl.multiple_of(tp * 512, 512), 512)]
    got(wo.at[pl.ds(0, 96), pl.ds(0, 512)], rsem.at[10])
    push(my_lanes, my_lanes, 11, {"tp": 1 - tp})
    got(fbuf.at[tp, y], fsem.at[4])
    first = fbuf.at[tp, below, 0]
    push(first, first, 12, at_y(above), fsem.at[6])
    got(fbuf.at[tp, y], fsem.at[5])
    second = fbuf.at[tp, above, 1]
    push(second, second, 12, at_y(below), fsem.at[7])
    push(fbuf.at[tp, below], fbuf.at[tp, below], 7, {"tp": 1 - tp}, fsem.at[8])
    push(fbuf.at[tp, above], fbuf.at[tp, above], 7, {"tp": 1 - tp}, fsem.at[8])

    @pl.when(half == tp)
    def _():
        got(nrecv.at[pl.ds(0, 15)], rsem.at[5])

    @pl.when(half != tp)
    def _():
        got(nrecv, rsem.at[5])

    got(my_lanes, rsem.at[11])
    nf[...] = nrecv[...].astype(F32).reshape(256, 128)
    wide = jnp.concatenate(
        [
            jnp.concatenate(
                [nf[pl.ds(t * 16 + h * 3 + i, 8, 32), :] for i in range(3)], axis=0
            )
            for t in range(2)
            for h in range(4)
        ],
        axis=1,
    ).astype(BF16)
    mixed = lax.dot_general(wide, wo[...], NT, preferred_element_type=F32)
    mine = jnp.concatenate(
        [xs[pl.ds(pl.multiple_of(i * 16 + tp * 8, 8), 8), :] for i in range(3)], axis=0
    )
    resid = (mine + mixed).astype(BF16).astype(F32)
    res[...] = resid
    scaled2 = (resid * xs[49:50, :]).astype(BF16).astype(F32)
    total = lax.dot_general(
        jnp.ones((8, 128), F32),
        jnp.concatenate([resid * resid, jnp.zeros((104, 128), F32)], axis=0),
        NT,
        preferred_element_type=F32,
        precision=lax.Precision.HIGHEST,
    )
    total_hi = total.astype(BF16).astype(F32)
    r8 = iota((8, 128), 0)
    tail = jnp.where(r8 == 0, total_hi, jnp.where(r8 == 1, total - total_hi, 0.0))
    rsend[...] = jnp.concatenate([scaled2, tail], axis=0).astype(BF16)
    along(lambda far: rsend, rrecv.at[z], 6)
    rrecv[z] = rsend[...]
    got(first, fsem.at[6])
    got(second, fsem.at[7])
    push(fbuf.at[tp, across], fbuf.at[tp, across], 7, {"tp": 1 - tp}, fsem.at[8])
    got(rrecv.at[pl.ds(0, NZ - 1)], rsem.at[6])
    rows = jnp.concatenate([rrecv[k] for k in range(NZ)], axis=1)
    sums = rrecv[0, 16:32, :].astype(F32)
    for k in range(1, NZ):
        sums = sums + rrecv[k, 16:32, :].astype(F32)
    squares = sums[8:9] + sums[9:10]
    scale = lax.rsqrt(squares / D + 1e-06)
    dr, dc = iota((R3, 128), 0), iota((R3, 128), 1)
    scale = jnp.sum(jnp.where(dr == dc, scale, 0.0), axis=1, keepdims=True)
    got(fbuf.at[0], fsem.at[8])
    up_w = fbuf[:, :, 0].reshape(512, D)
    up = lax.dot_general(rows, up_w, NT, preferred_element_type=F32) * scale
    act = jnp.square(jnp.maximum(up, 0.0)).astype(BF16)
    for k in range(NZ // 2):
        part = jnp.dot(
            act,
            fbuf[:, :, 1, :, k * 256 : (k + 1) * 256].reshape(512, 256),
            preferred_element_type=F32,
        ).astype(BF16)
        dsend[2 * k] = part[:24, :128]
        dsend[2 * k + 1] = part[:24, 128:]
    along(lambda far: dsend.at[far], drecv.at[z], 8)
    drecv[z] = dsend[z]
    got(drecv.at[pl.ds(0, NZ - 1)], rsem.at[8])
    final = res[...]
    for k in range(NZ):
        final = final + drecv[k].astype(F32)
    final = jnp.concatenate([final, jnp.zeros((104, 128), F32)], axis=0).T
    ysend[...] = final.astype(BF16).reshape(8, 16, 128)
    to_eight(lambda p: ysend.at[p], yrecv.at[me8], 9)
    yrecv[me8] = ysend[me8]
    got(yrecv.at[pl.ds(0, 7)], rsem.at[9])
    pieces = jnp.concatenate([yrecv[k] for k in range(8)], axis=1)
    placed = jnp.dot(pieces, qbuf[...], preferred_element_type=F32)
    out_ref[...] = placed[:, :192].astype(BF16)

    got(tbuf.at[pl.ds(0, 7)], ssem.at[0])
    got(wbuf.at[pl.ds(0, 2)], ssem.at[1])
    got(wbuf.at[0], ssem.at[2])
    got(wo.at[pl.ds(0, 96), pl.ds(0, 512)], ssem.at[10])
    got(wo.at[:, pl.ds(0, 512)], ssem.at[11])
    got(fbuf.at[tp, pl.ds(0, 2)], ssem.at[3])
    got(fbuf.at[tp, y], ssem.at[12])
    got(zsend.at[pl.ds(0, NZ - 1)], ssem.at[4])

    @pl.when(half == tp)
    def _():
        got(nrecv.at[pl.ds(0, 15)], ssem.at[5])

    @pl.when(half != tp)
    def _():
        got(nrecv, ssem.at[5])

    got(rrecv.at[pl.ds(0, NZ - 1)], ssem.at[6])
    got(fbuf.at[tp], ssem.at[7])
    got(dsend.at[pl.ds(0, NZ - 1)], ssem.at[8])
    got(ysend.at[pl.ds(0, 7)], ssem.at[9])


def finish(vec_ref, early_ref, state_hbm, out_ref, state_out, st, vt, load_sem, store_sem):
    loads = [
        pltpu.make_async_copy(state_hbm.at[i], st.at[i], load_sem.at[i]) for i in range(3)
    ]
    stores = [
        pltpu.make_async_copy(st.at[i], state_out.at[i], store_sem.at[i]) for i in range(3)
    ]
    for c in loads:
        c.start()
    out_ref[...] = early_ref[...]
    vt[...] = jnp.concatenate([vec_ref[0:16, :], jnp.zeros((112, 128), F32)], axis=0).T
    for i in range(3):
        loads[i].wait()
        for h in range(4):
            r = h * 3 + i
            kept = st[i, h] * vec_ref[24 + r : 25 + r, :]
            st[i, h] = kept + vt[:, r : r + 1] * vec_ref[12 + r : 13 + r, :]
        stores[i].start()
    for c in stores:
        c.wait()


def local_step(
    tokens,
    state,
    mix_gain,
    w_query,
    w_key,
    w_value,
    w_beta,
    w_decay,
    decay_log,
    head_gain,
    w_out,
    ff_gain,
    w_up,
    w_down,
):
    anywhere = pl.BlockSpec(memory_space=pltpu.HBM)
    vmem = pl.BlockSpec(memory_space=pltpu.VMEM)
    early, vec = pl.pallas_call(
        body,
        name="layer",
        out_shape=(
            jax.ShapeDtypeStruct((16, 192), BF16),
            jax.ShapeDtypeStruct((40, 128), F32),
        ),
        in_specs=[anywhere] * 14,
        out_specs=(vmem, vmem),
        scratch_shapes=[
            pltpu.VMEM((16, 192), BF16),
            pltpu.VMEM((1, 16), BF16),
            pltpu.VMEM((1, 16), BF16),
            pltpu.VMEM((4, 32), BF16),
            pltpu.VMEM((4, 32), BF16),
            pltpu.VMEM((1, 128), BF16),
            pltpu.VMEM((1, 4), F32),
            pltpu.VMEM((8, 16, 256), BF16),
            pltpu.VMEM((NY, 3, 32, 512), BF16),
            pltpu.VMEM((128, 1024), BF16),
            pltpu.VMEM((2, NY, 2, 64, D), BF16),
            pltpu.VMEM((3, 4, 128, 128), F32),
            pltpu.VMEM((1024, 256), BF16),
            pltpu.VMEM((1024, 128), BF16),
            pltpu.VMEM((56, 128), F32),
            pltpu.VMEM((NZ * R1, 128), F32),
            pltpu.VMEM((NZ, R1, 128), BF16),
            pltpu.VMEM((NZ, R1, 128), BF16),
            pltpu.VMEM((R1, 128), F32),
            pltpu.VMEM((24, 128), F32),
            pltpu.VMEM((16, 128), F32),
            pltpu.VMEM((16, 128), BF16),
            pltpu.VMEM((16, 16, 128), BF16),
            pltpu.VMEM((256, 128), F32),
            pltpu.VMEM((R3, 128), BF16),
            pltpu.VMEM((NZ, R3, 128), BF16),
            pltpu.VMEM((24, 128), F32),
            pltpu.VMEM((NZ, 24, 128), BF16),
            pltpu.VMEM((NZ, 24, 128), BF16),
            pltpu.VMEM((8, 16, 128), BF16),
            pltpu.VMEM((8, 16, 128), BF16),
            pltpu.SemaphoreType.DMA((14,)),
            pltpu.SemaphoreType.DMA((13,)),
            pltpu.SemaphoreType.DMA((13,)),
            pltpu.SemaphoreType.DMA((9,)),
            pltpu.SemaphoreType.REGULAR,
            pltpu.SemaphoreType.REGULAR,
            pltpu.SemaphoreType.REGULAR,
        ],
        compiler_params=pltpu.CompilerParams(
            collective_id=0, has_side_effects=True, vmem_limit_bytes=67043328
        ),
    )(
        tokens.T,
        mix_gain[None, :],
        ff_gain[None, :],
        w_beta.T,
        w_decay.T,
        head_gain[None, :],
        decay_log[None, :],
        state,
        w_query,
        w_key,
        w_value,
        w_out.T,
        w_up.T,
        w_down,
    )
    out, new_state = pl.pallas_call(
        finish,
        name="finish",
        out_shape=(
            jax.ShapeDtypeStruct((16, 192), BF16),
            jax.ShapeDtypeStruct(state.shape, F32),
        ),
        in_specs=[vmem, vmem, anywhere],
        out_specs=(vmem, anywhere),
        scratch_shapes=[
            pltpu.VMEM((3, 4, 128, 128), F32),
            pltpu.VMEM((128, 128), F32),
            pltpu.SemaphoreType.DMA((3,)),
            pltpu.SemaphoreType.DMA((3,)),
        ],
        compiler_params=pltpu.CompilerParams(vmem_limit_bytes=67043328),
    )(vec, early, state)
    return out.T, new_state


def solution(mesh):
    placed = (
        P("dp", ("kv", "tp")),
        P(("dp", "kv"), "tp", None, None),
        P(("kv", "tp")),
        P("kv", "tp"),
        P("kv", "tp"),
        P("kv", "tp"),
        P("kv", "tp"),
        P("kv", "tp"),
        P("tp"),
        P(),
        P("tp", "kv"),
        P(("kv", "tp")),
        P(None, ("kv", "tp")),
        P(("kv", "tp"), None),
    )
    return jax.shard_map(
        local_step,
        mesh=mesh,
        in_specs=placed,
        out_specs=(P("dp", ("kv", "tp")), P(("dp", "kv"), "tp", None, None)),
        check_vma=False,
    )
```

```python
import functools

import jax
import jax.numpy as jnp
from jax import lax
from jax.experimental import pallas as pl
from jax.experimental.pallas import tpu as pltpu
from jax.sharding import PartitionSpec as P

D = 2048
NZ = 16
NY = 4
MESH = pl.DeviceIdType.MESH
F32 = jnp.float32
BF16 = jnp.bfloat16
NT = (((1,), (1,)), ((), ()))
R1 = 40
GATE_AT = 200


def iota(shape, dim):
    return lax.broadcasted_iota(jnp.int32, shape, dim)


def body(
    tokens_hbm,
    mix_gain_hbm,
    ff_gain_hbm,
    beta_hbm,
    decay_hbm,
    head_gain_hbm,
    decay_log_hbm,
    state_hbm,
    wq_hbm,
    wk_hbm,
    wv_hbm,
    wo_hbm,
    wu_hbm,
    wd_hbm,
    out_ref,
    vec_ref,
    tok,
    mixg,
    ffg,
    bta,
    dcy,
    hgain,
    dlog,
    tbuf,
    wbuf,
    wo,
    fbuf,
    st,
    qbuf,
    ebuf,
    xs,
    zs,
    zsend,
    zrecv,
    accs,
    g12,
    hs,
    nsend,
    nrecv,
    nf,
    xrecv,
    rrecv,
    srecv,
    xw,
    res,
    dsend,
    drecv,
    ysend,
    yrecv,
    lsem,
    ssem,
    rsem,
    fsem,
    near_sem,
    mid_sem,
    far_sem,
):
    kv = lax.axis_index("kv")
    tp = lax.axis_index("tp")
    z = kv // NY
    y = kv % NY
    me8 = y * 2 + tp
    half = z // 8

    barrier = pltpu.get_barrier_semaphore()

    def local(src, dst, k):
        return pltpu.make_async_copy(src, dst, lsem.at[k])

    def mine(block):
        return wo.at[
            block,
            pl.ds(pl.multiple_of(y * 32, 32), 32),
            pl.ds(pl.multiple_of(tp * 512, 512), 512),
        ]

    loads = [
        local(wq_hbm, wbuf.at[y, 0], 5),
        local(wk_hbm, wbuf.at[y, 1], 6),
        local(wv_hbm, wbuf.at[y, 2], 7),
        local(tokens_hbm, tok, 0),
        local(mix_gain_hbm, mixg, 1),
        local(ff_gain_hbm, ffg, 2),
        local(beta_hbm, bta, 3),
        local(decay_hbm, dcy, 4),
        local(wo_hbm, mine(0), 8),
        local(wu_hbm, fbuf.at[tp, y, 0], 9),
        local(wd_hbm, fbuf.at[tp, y, 1], 10),
        local(head_gain_hbm, hgain, 11),
        local(decay_log_hbm, dlog, 12),
        local(state_hbm, st, 13),
    ]
    for c in loads:
        c.start()

    def greet(sem, where):
        pl.semaphore_signal(sem, inc=1, device_id=where, device_id_type=MESH)

    def on_ring(d):
        return {"kv": ((z + d) % NZ) * NY + y}

    def greet_eight(j, carry):
        p = (me8 + j) % 8
        greet(barrier, {"kv": z * NY + p // 2, "tp": p % 2})
        return carry

    lax.fori_loop(1, 8, greet_eight, 0)
    greet(barrier, on_ring(1))
    greet(barrier, on_ring(NZ - 1))

    for c in loads[:3]:
        c.wait()

    pl.semaphore_wait(barrier, 9)

    def push(src, dst, k, where, to=None):
        pltpu.make_async_remote_copy(
            src_ref=src,
            dst_ref=dst,
            send_sem=ssem.at[k],
            recv_sem=rsem.at[k] if to is None else to,
            device_id=where,
            device_id_type=MESH,
        ).start()

    def to_eight(src_of, dst, k):
        def one(j, carry):
            p = (me8 + j) % 8
            push(src_of(p), dst, k, {"kv": z * NY + p // 2, "tp": p % 2})
            return carry

        lax.fori_loop(1, 8, one, 0)

    above, below, across = (y + 1) % NY, (y + NY - 1) % NY, (y + 2) % NY

    sibling = {"tp": 1 - tp}

    def at_y(other):
        return {"kv": z * NY + other}

    def got(ref, sem):
        pltpu.make_async_copy(ref, ref, sem).wait()

    high, low = pl.ds(0, 16), pl.ds(16, 16)
    for part, k in ((high, 0), (low, 1)):
        push(wbuf.at[y, :, part], wbuf.at[y, :, part], 1, at_y(above), fsem.at[k])
    for part, k in ((low, 2), (high, 3)):
        push(wbuf.at[y, :, part], wbuf.at[y, :, part], 1, at_y(below), fsem.at[k])
    greet(near_sem, on_ring(1))
    greet(near_sem, on_ring(NZ - 1))

    row, col = iota((56, 256), 0), iota((56, 256), 1)
    wanted = jnp.where(row < 48, 12 * (row % 16) + 3 * y + row // 16, row + 144)
    pick = jnp.where((col == wanted) & (row < 50), 1.0, 0.0).astype(BF16)

    pr, pc = iota((32, 256), 0), iota((32, 256), 1)
    shift = jnp.where(pc == pr + GATE_AT, 1.0, 0.0).astype(BF16)

    for c in loads[3:8]:
        c.wait()
    sr, sc = iota((16, 16), 0), iota((16, 16), 1)

    def upright(ref):
        return jnp.sum(jnp.where(sr == sc, ref[...].astype(F32), 0.0), axis=1, keepdims=True)

    gate_rows = jnp.concatenate([bta[...].astype(F32), dcy[...].astype(F32)], axis=0)
    gate_rows = jnp.concatenate([gate_rows, jnp.zeros((8, 32), F32)], axis=0).astype(BF16)
    lanes = iota((16, 256), 1)
    tile = jnp.dot(gate_rows, shift, preferred_element_type=F32)
    tile = jnp.where(lanes == 192, upright(mixg), jnp.where(lanes == 193, upright(ffg), tile))
    tile = tile + jnp.concatenate([tok[...].astype(F32), jnp.zeros((16, 64), F32)], axis=1)
    tbuf[me8] = tile.astype(BF16)
    to_eight(lambda p: tbuf.at[me8], tbuf.at[me8], 0)
    pl.semaphore_wait(near_sem, 2)
    greet(mid_sem, on_ring(2))
    greet(mid_sem, on_ring(NZ - 2))
    er, ec = iota((1024, 128), 0), iota((1024, 128), 1)
    into = er % 256 - GATE_AT
    spread = jnp.where((ec == er // 256 * 32 + into) & (into >= 0) & (into < 32), 1.0, 0.0)
    ebuf[...] = spread.astype(BF16)
    pl.semaphore_wait(mid_sem, 2)
    greet(far_sem, on_ring(4))
    greet(far_sem, on_ring(NZ - 4))
    for c in loads[8:11]:
        c.wait()
    push(mine(0), mine(3), 10, on_ring(4))
    push(mine(0), mine(1), 10, on_ring(NZ - 4))
    got(wbuf.at[y, :, high], fsem.at[0])
    push(wbuf.at[below, :, high], wbuf.at[below, :, high], 2, at_y(above), fsem.at[4])
    got(wbuf.at[y, :, low], fsem.at[2])
    push(wbuf.at[above, :, low], wbuf.at[above, :, low], 2, at_y(below), fsem.at[5])
    for other, k in ((above, 6), (below, 7)):
        push(fbuf.at[tp, y, 0], fbuf.at[tp, y, 0], 3, at_y(other), fsem.at[k])
    push(fbuf.at[tp, y], fbuf.at[tp, y], 7, sibling, fsem.at[12])
    pl.semaphore_wait(far_sem, 2)
    push(mine(0), mine(2), 10, on_ring(8))
    got(tbuf.at[pl.ds(0, 7)], rsem.at[0])
    tiles = tbuf[...]
    turned = tiles.reshape(128, 256)
    chosen = lax.dot_general(pick, turned, NT, preferred_element_type=F32)
    xs[...] = chosen
    gain_rows = jnp.where(iota((8, 128), 0) == 0, chosen[49:50], 0.0)
    token_rows = [xs[pl.ds(pl.multiple_of(i * 16 + tp * 8, 8), 8), :] for i in range(3)]
    xrecv[0] = jnp.concatenate(token_rows + [gain_rows], axis=0).astype(BF16)
    push(xrecv.at[0], xrecv.at[3], 8, on_ring(4))
    push(xrecv.at[0], xrecv.at[1], 8, on_ring(NZ - 4))
    push(xrecv.at[0], xrecv.at[2], 8, on_ring(8))
    x = chosen[:48]
    scaled = (x * chosen[48:49]).astype(BF16)
    square = jnp.sum(x * x, axis=1, keepdims=True)
    square_hi = square.astype(BF16).astype(F32)
    own = jnp.concatenate([tbuf[2 * k + tp] for k in range(NY)], axis=1)
    gate_w = jnp.dot(own, ebuf[...], preferred_element_type=F32)
    gate_w = jnp.where(iota((16, 128), 0) < 8, gate_w, 0.0).astype(BF16)
    gate_w = jnp.concatenate([gate_w, jnp.zeros((112, 128), BF16)], axis=0)
    gate = lax.dot_general(scaled, gate_w, NT, preferred_element_type=F32)
    gl = iota((48, 128), 1)
    gate = jnp.where(gl == 8, square_hi, jnp.where(gl == 9, square - square_hi, gate))

    got(wbuf.at[y, :, low], fsem.at[1])
    got(wbuf.at[y, :, high], fsem.at[3])
    got(wbuf.at[y, :, high], fsem.at[4])
    got(wbuf.at[y, :, low], fsem.at[5])
    for m in range(3):
        weight = wbuf[:, m].reshape(128, 512)
        part = jnp.dot(scaled, weight, preferred_element_type=F32)
        for h in range(4):
            for i in range(3):
                zs[pl.ds(m * 12 + h * 3 + i, NZ, R1), :] = part[
                    i * 16 : (i + 1) * 16, h * 128 : (h + 1) * 128
                ]
    for i in range(3):
        zs[pl.ds(36 + i, NZ, R1), :] = gate[i * 16 : (i + 1) * 16]
    zs[pl.ds(39, NZ, R1), :] = jnp.zeros((NZ, 128), F32)
    zsend[...] = zs[...].reshape(NZ, R1, 128).astype(BF16)

    def along(src_of, dst, k):
        def one(n, carry):
            d = NZ // 2 + ((n + 1) // 2) * (1 - 2 * (n % 2))
            far = (z + d) % NZ
            push(src_of(far), dst, k, {"kv": far * NY + y})
            return carry

        lax.fori_loop(0, NZ - 1, one, 0)

    along(lambda far: zsend.at[far], zrecv.at[z], 4)
    zrecv[z] = zsend[z]
    for c in loads[11:]:
        c.wait()
    src_row, seq_col = iota((1024, 256), 0), iota((1024, 256), 1)
    lane = src_row % 128
    place = 12 * ((src_row // 128 % 2) * 8 + lane % 8) + 3 * (src_row // 256) + lane // 8
    qbuf[...] = jnp.where((seq_col == place) & (lane < 24), 1.0, 0.0).astype(BF16)

    def column(other, blocks):
        return wo.at[
            blocks,
            pl.ds(pl.multiple_of(other * 32, 32), 32),
            pl.ds(pl.multiple_of(tp * 512, 512), 512),
        ]

    every, first, last = pl.ds(0, 4), pl.ds(0, 2), pl.ds(2, 2)
    got(column(y, pl.ds(0, 3)), rsem.at[10])
    for other, k in ((above, 8), (below, 9)):
        push(column(y, every), column(y, every), 11, at_y(other), fsem.at[k])
    for other, k in ((above, 10), (below, 11)):
        push(fbuf.at[tp, y, 1], fbuf.at[tp, y, 1], 3, at_y(other), fsem.at[k])
    got(zrecv.at[pl.ds(0, NZ - 1)], rsem.at[4])

    acc = zrecv[0].astype(F32)
    for k in range(1, NZ):
        acc = acc + zrecv[k].astype(F32)
    accs[...] = acc
    for h in range(4):
        g12[3 * h : 3 * h + 3, :] = accs[36:39, :]
    g = g12[0:12, :]
    r12, l12 = iota((12, 128), 0), iota((12, 128), 1)
    head_of = r12 // 3

    def take(mask):
        return jnp.sum(jnp.where(mask, g, 0.0), axis=1, keepdims=True)

    inverse = lax.rsqrt(take((l12 == 8) | (l12 == 9)) / D + 1e-06)
    beta = jax.nn.sigmoid(inverse * take(l12 == head_of))
    u = inverse * take(l12 == head_of + 4)
    soft = jnp.maximum(u, 0.0) + jnp.log1p(jnp.exp(-jnp.abs(u)))
    lr, lc = iota((12, 4), 0), iota((12, 4), 1)
    rate = jnp.sum(jnp.where(lc == lr // 3, dlog[...], 0.0), axis=1, keepdims=True)
    keep = jnp.exp(-jnp.exp(rate) * soft)
    query = inverse * accs[0:12, :]
    key = inverse * accs[12:24, :]
    value = inverse * accs[24:36, :]
    qnorm = query * lax.rsqrt(jnp.sum(query * query, axis=1, keepdims=True) + 1e-06)
    knorm = key * lax.rsqrt(jnp.sum(key * key, axis=1, keepdims=True) + 1e-06)
    pad = jnp.zeros((104, 128), F32)
    g12[0:12, :] = qnorm
    g12[12:24, :] = knorm
    both = jnp.concatenate([g12[...], pad], axis=0).T
    for r in range(12):
        h, i = r // 3, r % 3
        kc = both[:, 12 + r : 13 + r]
        qc = both[:, r : r + 1]
        kept = st[i, h] * keep[r : r + 1, :]
        predicted = jnp.sum(kept * kc, axis=0, keepdims=True)
        change = beta[r : r + 1, :] * (value[r : r + 1, :] - predicted)
        vec_ref[12 + r : 13 + r, :] = change
        hs[r : r + 1, :] = jnp.sum((kept + kc * change) * qc, axis=0, keepdims=True)
    vec_ref[0:12, :] = knorm
    vec_ref[24:36, :] = jnp.broadcast_to(keep, (12, 128))
    heads = hs[...] / jnp.sqrt(jnp.float32(128))
    heads = jnp.where(iota((16, 128), 0) < 12, heads, 0.0)
    normed = (
        heads
        * lax.rsqrt(jnp.mean(heads * heads, axis=1, keepdims=True) + 1e-06)
        * hgain[...].astype(F32)
    )
    nsend[...] = normed.astype(BF16)

    slot = (z % 8) * 2 + tp

    def spread_heads(n, carry):
        d = (NZ // 2 + ((n + 1) // 2) * (1 - 2 * (n % 2))) % NZ
        far = (z + d) % NZ
        push(nsend, nrecv.at[slot], 5, {"kv": far * NY + y, "tp": half})
        return carry

    lax.fori_loop(0, NZ - 1, spread_heads, 0)

    @pl.when(half == tp)
    def _():
        nrecv[slot] = nsend[...]

    @pl.when(half != tp)
    def _():
        push(nsend, nrecv.at[slot], 5, {"tp": half})

    ahead, behind = pl.ds(0, 32), pl.ds(32, 32)
    got(column(y, every), fsem.at[8])
    push(column(below, first), column(below, first), 2, at_y(above), fsem.at[13])
    got(column(y, every), fsem.at[9])
    push(column(above, last), column(above, last), 2, at_y(below), fsem.at[14])
    for m, (a, b, c, d) in ((0, (6, 7, 15, 16)), (1, (10, 11, 17, 18))):
        got(fbuf.at[tp, y, m], fsem.at[a])
        push(
            fbuf.at[tp, below, m, ahead], fbuf.at[tp, below, m, ahead], 9, at_y(above), fsem.at[c]
        )
        got(fbuf.at[tp, y, m], fsem.at[b])
        push(
            fbuf.at[tp, above, m, behind],
            fbuf.at[tp, above, m, behind],
            9,
            at_y(below),
            fsem.at[d],
        )
        for other in (above, below):
            push(fbuf.at[tp, other, m], fbuf.at[tp, other, m], 7, sibling, fsem.at[12])
    got(column(y, first), fsem.at[13])
    got(column(y, last), fsem.at[14])
    my_lanes = wo.at[:, :, pl.ds(pl.multiple_of(tp * 512, 512), 512)]
    push(my_lanes, my_lanes, 12, sibling)
    @pl.when(half == tp)
    def _():
        got(nrecv.at[pl.ds(0, 15)], rsem.at[5])

    @pl.when(half != tp)
    def _():
        got(nrecv, rsem.at[5])

    got(my_lanes, rsem.at[12])
    got(xrecv.at[pl.ds(0, 3)], rsem.at[8])
    nf[...] = nrecv[...].astype(F32).reshape(256, 128)
    wide = jnp.concatenate(
        [
            jnp.concatenate(
                [nf[pl.ds(t * 16 + h * 3 + i, 8, 32), :] for i in range(3)], axis=0
            )
            for t in range(2)
            for h in range(4)
        ],
        axis=1,
    ).astype(BF16)
    spent = jnp.zeros((24, 128), F32)
    for j in range(4):
        mixed = lax.dot_general(wide, wo[j], NT, preferred_element_type=F32)
        known = xrecv[j].astype(F32)
        resid = (known[:24] + mixed).astype(BF16).astype(F32)
        if j == 0:
            res[...] = resid
        rrecv[0, j] = (resid * known[24:25]).astype(BF16)
        spent = spent + resid * resid
    total = lax.dot_general(
        jnp.ones((8, 128), F32),
        jnp.concatenate([spent, jnp.zeros((104, 128), F32)], axis=0),
        NT,
        preferred_element_type=F32,
        precision=lax.Precision.HIGHEST,
    )
    total_hi = total.astype(BF16).astype(F32)
    r8 = iota((8, 128), 0)
    tail = jnp.where(r8 == 0, total_hi, jnp.where(r8 == 1, total - total_hi, 0.0))
    srecv[0] = tail.astype(BF16)
    for slot_at, d in ((3, NZ - 2), (1, NZ - 1), (2, 1)):
        push(rrecv.at[0], rrecv.at[slot_at], 6, on_ring(d))
        push(srecv.at[0], srecv.at[slot_at], 5, on_ring(d), rsem.at[7])
    for m, (a, b) in ((0, (15, 16)), (1, (17, 18))):
        got(fbuf.at[tp, y, m, ahead], fsem.at[a])
        got(fbuf.at[tp, y, m, behind], fsem.at[b])
        push(fbuf.at[tp, across, m], fbuf.at[tp, across, m], 7, sibling, fsem.at[12])
    got(rrecv.at[pl.ds(0, 3)], rsem.at[6])
    got(srecv.at[pl.ds(0, 3)], rsem.at[7])
    for k, off in enumerate((0, 1, NZ - 1, 2)):
        for j in range(4):
            at = pl.multiple_of((z + off + 4 * j) % NZ * 128, 128)
            xw[:, pl.ds(at, 128)] = rrecv[k, j]
    sums = srecv[0].astype(F32)
    for k in range(1, 4):
        sums = sums + srecv[k].astype(F32)
    squares = sums[0:1] + sums[1:2]
    scale = lax.rsqrt(squares / D + 1e-06)
    dr, dc = iota((24, 128), 0), iota((24, 128), 1)
    scale = jnp.sum(jnp.where(dr == dc, scale, 0.0), axis=1, keepdims=True)
    got(fbuf.at[0], fsem.at[12])
    up_w = fbuf[:, :, 0].reshape(512, D)
    up = lax.dot_general(xw[...], up_w, NT, preferred_element_type=F32) * scale
    act = jnp.square(jnp.maximum(up, 0.0)).astype(BF16)
    for group in ((8, 7, 9, 6), (10, 5, 11, 4), (12, 3, 13, 2), (14, 1, 15, 0)):
        away = [(z + d) % NZ for d in group]
        down_w = jnp.concatenate(
            [
                fbuf[:, :, 1, :, pl.ds(pl.multiple_of(far * 128, 128), 128)].reshape(512, 128)
                for far in away
            ],
            axis=1,
        )
        part = jnp.dot(act, down_w, preferred_element_type=F32).astype(BF16)
        for n, (d, far) in enumerate(zip(group, away)):
            dsend[far] = part[:, n * 128 : (n + 1) * 128]
            if d:
                push(dsend.at[far], drecv.at[z], 13, {"kv": far * NY + y})
    drecv[z] = dsend[z]
    got(drecv.at[pl.ds(0, NZ - 1)], rsem.at[13])
    final = res[...]
    for k in range(NZ):
        final = final + drecv[k].astype(F32)
    final = jnp.concatenate([final, jnp.zeros((104, 128), F32)], axis=0).T
    ysend[...] = final.astype(BF16).reshape(8, 16, 128)
    to_eight(lambda p: ysend.at[p], yrecv.at[me8], 14)
    yrecv[me8] = ysend[me8]
    got(yrecv.at[pl.ds(0, 7)], rsem.at[14])
    pieces = jnp.concatenate([yrecv[k] for k in range(8)], axis=1)
    placed = jnp.dot(pieces, qbuf[...], preferred_element_type=F32)
    out_ref[...] = placed[:, :192].astype(BF16)

    got(tbuf.at[pl.ds(0, 7)], ssem.at[0])
    got(wbuf.at[pl.ds(0, 2)], ssem.at[1])
    got(wbuf.at[0], ssem.at[2])
    got(wo.at[pl.ds(0, 2), pl.ds(0, 64), pl.ds(0, 512)], ssem.at[2])
    got(fbuf.at[tp, pl.ds(0, 2)], ssem.at[3])
    got(zsend.at[pl.ds(0, NZ - 1)], ssem.at[4])

    @pl.when(half == tp)
    def _():
        got(nrecv.at[pl.ds(0, 15)], ssem.at[5])

    @pl.when(half != tp)
    def _():
        got(nrecv, ssem.at[5])

    got(srecv.at[pl.ds(0, 3)], ssem.at[5])
    got(rrecv.at[pl.ds(0, 3)], ssem.at[6])
    got(fbuf.at[tp], ssem.at[7])
    got(xrecv.at[pl.ds(0, 3)], ssem.at[8])
    got(fbuf.at[tp, y], ssem.at[9])
    got(column(y, pl.ds(0, 3)), ssem.at[10])
    got(column(y, every), ssem.at[11])
    got(column(y, every), ssem.at[11])
    got(my_lanes, ssem.at[12])
    got(dsend.at[pl.ds(0, NZ - 1)], ssem.at[13])
    got(ysend.at[pl.ds(0, 7)], ssem.at[14])


def finish(
    vec_hbm, early_hbm, state_hbm, out_hbm, state_out, st, vec, ob, vt, load_sem, store_sem, small
):
    pairs = [(i, h) for i in range(3) for h in range(4)]
    first = pltpu.make_async_copy(vec_hbm, vec, small.at[0])
    early = pltpu.make_async_copy(early_hbm, ob, small.at[1])
    late = pltpu.make_async_copy(ob, out_hbm, small.at[2])
    loads = [
        pltpu.make_async_copy(state_hbm.at[i, h], st.at[i, h], load_sem.at[i, h]) for i, h in pairs
    ]
    stores = [
        pltpu.make_async_copy(st.at[i, h], state_out.at[i, h], store_sem.at[i, h]) for i, h in pairs
    ]
    for c in [first, early] + loads:
        c.start()
    first.wait()
    vt[...] = jnp.concatenate([vec[0:16, :], jnp.zeros((112, 128), F32)], axis=0).T
    for n, (i, h) in enumerate(pairs):
        r = h * 3 + i
        loads[n].wait()
        kept = st[i, h] * vec[24 + r : 25 + r, :]
        st[i, h] = kept + vt[:, r : r + 1] * vec[12 + r : 13 + r, :]
        stores[n].start()
    early.wait()
    late.start()
    for c in stores + [late]:
        c.wait()


def local_step(
    tokens,
    state,
    mix_gain,
    w_query,
    w_key,
    w_value,
    w_beta,
    w_decay,
    decay_log,
    head_gain,
    w_out,
    ff_gain,
    w_up,
    w_down,
):
    anywhere = pl.BlockSpec(memory_space=pltpu.HBM)
    vmem = pl.BlockSpec(memory_space=pltpu.VMEM)
    early, vec = pl.pallas_call(
        body,
        name="layer",
        out_shape=(
            jax.ShapeDtypeStruct((16, 192), BF16),
            jax.ShapeDtypeStruct((40, 128), F32),
        ),
        in_specs=[anywhere] * 14,
        out_specs=(vmem, vmem),
        scratch_shapes=[
            pltpu.VMEM((16, 192), BF16),
            pltpu.VMEM((1, 16), BF16),
            pltpu.VMEM((1, 16), BF16),
            pltpu.VMEM((4, 32), BF16),
            pltpu.VMEM((4, 32), BF16),
            pltpu.VMEM((1, 128), BF16),
            pltpu.VMEM((1, 4), F32),
            pltpu.VMEM((8, 16, 256), BF16),
            pltpu.VMEM((NY, 3, 32, 512), BF16),
            pltpu.VMEM((4, 128, 1024), BF16),
            pltpu.VMEM((2, NY, 2, 64, D), BF16),
            pltpu.VMEM((3, 4, 128, 128), F32),
            pltpu.VMEM((1024, 256), BF16),
            pltpu.VMEM((1024, 128), BF16),
            pltpu.VMEM((56, 128), F32),
            pltpu.VMEM((NZ * R1, 128), F32),
            pltpu.VMEM((NZ, R1, 128), BF16),
            pltpu.VMEM((NZ, R1, 128), BF16),
            pltpu.VMEM((R1, 128), F32),
            pltpu.VMEM((24, 128), F32),
            pltpu.VMEM((16, 128), F32),
            pltpu.VMEM((16, 128), BF16),
            pltpu.VMEM((16, 16, 128), BF16),
            pltpu.VMEM((256, 128), F32),
            pltpu.VMEM((4, 32, 128), BF16),
            pltpu.VMEM((4, 4, 24, 128), BF16),
            pltpu.VMEM((4, 8, 128), BF16),
            pltpu.VMEM((24, D), BF16),
            pltpu.VMEM((24, 128), F32),
            pltpu.VMEM((NZ, 24, 128), BF16),
            pltpu.VMEM((NZ, 24, 128), BF16),
            pltpu.VMEM((8, 16, 128), BF16),
            pltpu.VMEM((8, 16, 128), BF16),
            pltpu.SemaphoreType.DMA((14,)),
            pltpu.SemaphoreType.DMA((15,)),
            pltpu.SemaphoreType.DMA((15,)),
            pltpu.SemaphoreType.DMA((19,)),
            pltpu.SemaphoreType.REGULAR,
            pltpu.SemaphoreType.REGULAR,
            pltpu.SemaphoreType.REGULAR,
        ],
        compiler_params=pltpu.CompilerParams(
            collective_id=0, has_side_effects=True, vmem_limit_bytes=67043328
        ),
    )(
        tokens.T,
        mix_gain[None, :],
        ff_gain[None, :],
        w_beta.T,
        w_decay.T,
        head_gain[None, :],
        decay_log[None, :],
        state,
        w_query,
        w_key,
        w_value,
        w_out.T,
        w_up.T,
        w_down,
    )
    out, new_state = pl.pallas_call(
        finish,
        name="finish",
        out_shape=(
            jax.ShapeDtypeStruct((16, 192), BF16),
            jax.ShapeDtypeStruct(state.shape, F32),
        ),
        in_specs=[anywhere] * 3,
        out_specs=(anywhere, anywhere),
        scratch_shapes=[
            pltpu.VMEM((3, 4, 128, 128), F32),
            pltpu.VMEM((40, 128), F32),
            pltpu.VMEM((16, 192), BF16),
            pltpu.VMEM((128, 128), F32),
            pltpu.SemaphoreType.DMA((3, 4)),
            pltpu.SemaphoreType.DMA((3, 4)),
            pltpu.SemaphoreType.DMA((3,)),
        ],
        compiler_params=pltpu.CompilerParams(vmem_limit_bytes=67043328),
    )(vec, early, state)
    return out.T, new_state


def solution(mesh):
    placed = (
        P("dp", ("kv", "tp")),
        P(("dp", "kv"), "tp", None, None),
        P(("kv", "tp")),
        P("kv", "tp"),
        P("kv", "tp"),
        P("kv", "tp"),
        P("kv", "tp"),
        P("kv", "tp"),
        P("tp"),
        P(),
        P("tp", "kv"),
        P(("kv", "tp")),
        P(None, ("kv", "tp")),
        P(("kv", "tp"), None),
    )
    return jax.shard_map(
        local_step,
        mesh=mesh,
        in_specs=placed,
        out_specs=(P("dp", ("kv", "tp")), P(("dp", "kv"), "tp", None, None)),
        check_vma=False,
    )
```

```python
import functools

import jax
import jax.numpy as jnp
from jax import lax
from jax.experimental import pallas as pl
from jax.experimental.pallas import tpu as pltpu
from jax.sharding import PartitionSpec as P

D = 2048
NZ = 16
NY = 4
MESH = pl.DeviceIdType.MESH
F32 = jnp.float32
BF16 = jnp.bfloat16
NT = (((1,), (1,)), ((), ()))
R1 = 40
GATE_AT = 200
VMEM = 60 * 1024 * 1024


def iota(shape, dim):
    return lax.broadcasted_iota(jnp.int32, shape, dim)


def body(
    tokens_hbm,
    mix_gain_hbm,
    ff_gain_hbm,
    beta_hbm,
    decay_hbm,
    head_gain_hbm,
    decay_log_hbm,
    state_hbm,
    wq_hbm,
    wk_hbm,
    wv_hbm,
    wo_hbm,
    wu_hbm,
    wd_hbm,
    out_ref,
    state_out,
    tok,
    mixg,
    ffg,
    bta,
    dcy,
    hgain,
    dlog,
    tbuf,
    wbuf,
    wo,
    fbuf,
    st,
    qbuf,
    ebuf,
    xs,
    zs,
    zsend,
    zrecv,
    accs,
    g12,
    hs,
    nsend,
    nrecv,
    nf,
    rsend,
    rrecv,
    res,
    dsend,
    drecv,
    ysend,
    yrecv,
    lsem,
    ssem,
    rsem,
    fsem,
    near_sem,
    mid_sem,
    far_sem,
):
    kv = lax.axis_index("kv")
    tp = lax.axis_index("tp")
    z = kv // NY
    y = kv % NY
    me8 = y * 2 + tp
    half = z // 8

    barrier = pltpu.get_barrier_semaphore()

    def local(src, dst, k):
        return pltpu.make_async_copy(src, dst, lsem.at[k])

    mine = wo.at[
        pl.ds(pl.multiple_of(y * 32, 32), 32), pl.ds(pl.multiple_of(tp * 512, 512), 512)
    ]

    loads = [
        local(wq_hbm, wbuf.at[y, 0], 5),
        local(wk_hbm, wbuf.at[y, 1], 6),
        local(wv_hbm, wbuf.at[y, 2], 7),
        local(tokens_hbm, tok, 0),
        local(mix_gain_hbm, mixg, 1),
        local(ff_gain_hbm, ffg, 2),
        local(beta_hbm, bta, 3),
        local(decay_hbm, dcy, 4),
        local(wo_hbm, mine, 8),
        local(wu_hbm, fbuf.at[tp, y, 0], 9),
        local(wd_hbm, fbuf.at[tp, y, 1], 10),
        local(head_gain_hbm, hgain, 11),
        local(decay_log_hbm, dlog, 12),
        local(state_hbm, st, 13),
    ]
    for c in loads[:3]:
        c.start()

    def greet(sem, where):
        pl.semaphore_signal(sem, inc=1, device_id=where, device_id_type=MESH)

    def on_ring(d):
        return {"kv": ((z + d) % NZ) * NY + y}

    def at_y(other):
        return {"kv": z * NY + other}

    above, below, across = (y + 1) % NY, (y + NY - 1) % NY, (y + 2) % NY
    sibling = {"tp": 1 - tp}
    beside = [at_y(above), at_y(below), on_ring(1), on_ring(NZ - 1)]
    diagonal = [{**at_y(above), **sibling}, {**at_y(below), **sibling}]
    for where in beside + [sibling] + diagonal:
        greet(barrier, where)
    for c in loads[3:]:
        c.start()

    for c in loads[:3]:
        c.wait()

    pl.semaphore_wait(barrier, 7)

    def push(src, dst, k, where, to=None):
        pltpu.make_async_remote_copy(
            src_ref=src,
            dst_ref=dst,
            send_sem=ssem.at[k],
            recv_sem=rsem.at[k] if to is None else to,
            device_id=where,
            device_id_type=MESH,
        ).start()

    def to_eight(src_of, dst, k):
        def one(j, carry):
            p = (me8 + j) % 8
            push(src_of(p), dst, k, {"kv": z * NY + p // 2, "tp": p % 2})
            return carry

        lax.fori_loop(1, 8, one, 0)

    def got(ref, sem):
        pltpu.make_async_copy(ref, ref, sem).wait()

    high, low = pl.ds(0, 16), pl.ds(16, 16)
    for part, k in ((high, 0), (low, 1)):
        push(wbuf.at[y, :, part], wbuf.at[y, :, part], 1, at_y(above), fsem.at[k])
    for part, k in ((low, 2), (high, 3)):
        push(wbuf.at[y, :, part], wbuf.at[y, :, part], 1, at_y(below), fsem.at[k])
    for where in beside:
        greet(near_sem, where)

    row, col = iota((56, 256), 0), iota((56, 256), 1)
    wanted = jnp.where(row < 48, 12 * (row % 16) + 3 * y + row // 16, row + 144)
    pick = jnp.where((col == wanted) & (row < 50), 1.0, 0.0).astype(BF16)

    pr, pc = iota((32, 256), 0), iota((32, 256), 1)
    shift = jnp.where(pc == pr + GATE_AT, 1.0, 0.0).astype(BF16)

    for c in loads[3:8]:
        c.wait()
    sr, sc = iota((16, 16), 0), iota((16, 16), 1)

    def upright(ref):
        return jnp.sum(jnp.where(sr == sc, ref[...].astype(F32), 0.0), axis=1, keepdims=True)

    gate_rows = jnp.concatenate([bta[...].astype(F32), dcy[...].astype(F32)], axis=0)
    gate_rows = jnp.concatenate([gate_rows, jnp.zeros((8, 32), F32)], axis=0).astype(BF16)
    lanes = iota((16, 256), 1)
    tile = jnp.dot(gate_rows, shift, preferred_element_type=F32)
    tile = jnp.where(lanes == 192, upright(mixg), jnp.where(lanes == 193, upright(ffg), tile))
    tile = tile + jnp.concatenate([tok[...].astype(F32), jnp.zeros((16, 64), F32)], axis=1)
    tbuf[me8] = tile.astype(BF16)
    pl.semaphore_wait(near_sem, 4)
    greet(mid_sem, on_ring(2))
    greet(mid_sem, on_ring(NZ - 2))
    to_eight(lambda p: tbuf.at[me8], tbuf.at[me8], 0)
    got(wbuf.at[y, :, high], fsem.at[0])
    push(wbuf.at[below, :, high], wbuf.at[below, :, high], 2, at_y(above), fsem.at[4])
    got(wbuf.at[y, :, low], fsem.at[2])
    push(wbuf.at[above, :, low], wbuf.at[above, :, low], 2, at_y(below), fsem.at[5])
    pl.semaphore_wait(mid_sem, 2)
    greet(far_sem, on_ring(4))
    greet(far_sem, on_ring(NZ - 4))
    for c in loads[8:11]:
        c.wait()
    for other in (above, below, across):
        push(mine, mine, 11, at_y(other), fsem.at[8])
    for m, (a, b) in ((0, (6, 7)), (1, (10, 11))):
        push(fbuf.at[tp, y, m], fbuf.at[tp, y, m], 3, at_y(above), fsem.at[a])
        push(fbuf.at[tp, y, m], fbuf.at[tp, y, m], 3, at_y(below), fsem.at[b])
    push(fbuf.at[tp, y], fbuf.at[tp, y], 7, sibling, fsem.at[12])
    er, ec = iota((1024, 128), 0), iota((1024, 128), 1)
    into = er % 256 - GATE_AT
    spread = jnp.where((ec == er // 256 * 32 + into) & (into >= 0) & (into < 32), 1.0, 0.0)
    ebuf[...] = spread.astype(BF16)
    got(tbuf.at[pl.ds(0, 7)], rsem.at[0])
    tiles = tbuf[...]
    turned = tiles.reshape(128, 256)
    chosen = lax.dot_general(pick, turned, NT, preferred_element_type=F32)
    xs[...] = chosen
    x = chosen[:48]
    scaled = (x * chosen[48:49]).astype(BF16)
    square = jnp.sum(x * x, axis=1, keepdims=True)
    square_hi = square.astype(BF16).astype(F32)
    own = jnp.concatenate([tbuf[2 * k + tp] for k in range(NY)], axis=1)
    gate_w = jnp.dot(own, ebuf[...], preferred_element_type=F32)
    gate_w = jnp.where(iota((16, 128), 0) < 8, gate_w, 0.0).astype(BF16)
    gate_w = jnp.concatenate([gate_w, jnp.zeros((112, 128), BF16)], axis=0)
    gate = lax.dot_general(scaled, gate_w, NT, preferred_element_type=F32)
    gl = iota((48, 128), 1)
    gate = jnp.where(gl == 8, square_hi, jnp.where(gl == 9, square - square_hi, gate))

    got(wbuf.at[y, :, low], fsem.at[1])
    got(wbuf.at[y, :, high], fsem.at[3])
    got(wbuf.at[y, :, high], fsem.at[4])
    got(wbuf.at[y, :, low], fsem.at[5])
    for m in range(3):
        weight = wbuf[:, m].reshape(128, 512)
        part = jnp.dot(scaled, weight, preferred_element_type=F32)
        for h in range(4):
            for i in range(3):
                zs[pl.ds(m * 12 + h * 3 + i, NZ, R1), :] = part[
                    i * 16 : (i + 1) * 16, h * 128 : (h + 1) * 128
                ]
    for i in range(3):
        zs[pl.ds(36 + i, NZ, R1), :] = gate[i * 16 : (i + 1) * 16]
    zs[pl.ds(39, NZ, R1), :] = jnp.zeros((NZ, 128), F32)
    zsend[...] = zs[...].reshape(NZ, R1, 128).astype(BF16)

    def along(src_of, dst, k):
        def one(n, carry):
            d = NZ // 2 + ((n + 1) // 2) * (1 - 2 * (n % 2))
            far = (z + d) % NZ
            push(src_of(far), dst, k, {"kv": far * NY + y})
            return carry

        lax.fori_loop(0, NZ - 1, one, 0)

    pl.semaphore_wait(far_sem, 2)
    along(lambda far: zsend.at[far], zrecv.at[z], 4)
    zrecv[z] = zsend[z]
    for c in loads[11:]:
        c.wait()
    src_row, seq_col = iota((1024, 256), 0), iota((1024, 256), 1)
    lane = src_row % 128
    place = 12 * ((src_row // 128 % 2) * 8 + lane % 8) + 3 * (src_row // 256) + lane // 8
    qbuf[...] = jnp.where((seq_col == place) & (lane < 24), 1.0, 0.0).astype(BF16)
    got(zrecv.at[pl.ds(0, NZ - 1)], rsem.at[4])

    acc = zrecv[0].astype(F32)
    for k in range(1, NZ):
        acc = acc + zrecv[k].astype(F32)
    accs[...] = acc
    for h in range(4):
        g12[3 * h : 3 * h + 3, :] = accs[36:39, :]
    g = g12[0:12, :]
    r12, l12 = iota((12, 128), 0), iota((12, 128), 1)
    head_of = r12 // 3

    def take(mask):
        return jnp.sum(jnp.where(mask, g, 0.0), axis=1, keepdims=True)

    inverse = lax.rsqrt(take((l12 == 8) | (l12 == 9)) / D + 1e-06)
    beta = jax.nn.sigmoid(inverse * take(l12 == head_of))
    u = inverse * take(l12 == head_of + 4)
    soft = jnp.maximum(u, 0.0) + jnp.log1p(jnp.exp(-jnp.abs(u)))
    lr, lc = iota((12, 4), 0), iota((12, 4), 1)
    rate = jnp.sum(jnp.where(lc == lr // 3, dlog[...], 0.0), axis=1, keepdims=True)
    keep = jnp.exp(-jnp.exp(rate) * soft)
    query = inverse * accs[0:12, :]
    key = inverse * accs[12:24, :]
    value = inverse * accs[24:36, :]
    qnorm = query * lax.rsqrt(jnp.sum(query * query, axis=1, keepdims=True) + 1e-06)
    knorm = key * lax.rsqrt(jnp.sum(key * key, axis=1, keepdims=True) + 1e-06)
    pad = jnp.zeros((104, 128), F32)
    g12[0:12, :] = qnorm
    g12[12:24, :] = knorm
    both = jnp.concatenate([g12[...], pad], axis=0).T
    for r in range(12):
        h, i = r // 3, r % 3
        kc = both[:, 12 + r : 13 + r]
        qc = both[:, r : r + 1]
        kept = st[i, h] * keep[r : r + 1, :]
        predicted = jnp.sum(kept * kc, axis=0, keepdims=True)
        change = beta[r : r + 1, :] * (value[r : r + 1, :] - predicted)
        new = kept + kc * change
        state_out[i, h] = new
        hs[r : r + 1, :] = jnp.sum(new * qc, axis=0, keepdims=True)
    heads = hs[...] / jnp.sqrt(jnp.float32(128))
    heads = jnp.where(iota((16, 128), 0) < 12, heads, 0.0)
    normed = (
        heads
        * lax.rsqrt(jnp.mean(heads * heads, axis=1, keepdims=True) + 1e-06)
        * hgain[...].astype(F32)
    )
    nsend[...] = normed.astype(BF16)

    slot = (z % 8) * 2 + tp

    def spread_heads(n, carry):
        d = (NZ // 2 + ((n + 1) // 2) * (1 - 2 * (n % 2))) % NZ
        far = (z + d) % NZ
        push(nsend, nrecv.at[slot], 5, {"kv": far * NY + y, "tp": half})
        return carry

    lax.fori_loop(0, NZ - 1, spread_heads, 0)

    @pl.when(half == tp)
    def _():
        nrecv[slot] = nsend[...]

    @pl.when(half != tp)
    def _():
        push(nsend, nrecv.at[slot], 5, {"tp": half})

    ahead, behind = pl.ds(0, 32), pl.ds(32, 32)
    got(wo.at[pl.ds(0, 96), pl.ds(0, 512)], fsem.at[8])
    my_lanes = wo.at[:, pl.ds(pl.multiple_of(tp * 512, 512), 512)]
    push(my_lanes, my_lanes, 12, sibling)
    for m, (a, b, c, d) in ((0, (6, 7, 15, 16)), (1, (10, 11, 17, 18))):
        got(fbuf.at[tp, y, m], fsem.at[a])
        push(
            fbuf.at[tp, below, m, ahead], fbuf.at[tp, below, m, ahead], 9, at_y(above), fsem.at[c]
        )
        got(fbuf.at[tp, y, m], fsem.at[b])
        push(
            fbuf.at[tp, above, m, behind],
            fbuf.at[tp, above, m, behind],
            9,
            at_y(below),
            fsem.at[d],
        )
        for other in (above, below):
            push(fbuf.at[tp, other, m], fbuf.at[tp, other, m], 7, sibling, fsem.at[12])
    @pl.when(half == tp)
    def _():
        got(nrecv.at[pl.ds(0, 15)], rsem.at[5])

    @pl.when(half != tp)
    def _():
        got(nrecv, rsem.at[5])

    got(my_lanes, rsem.at[12])
    nf[...] = nrecv[...].astype(F32).reshape(256, 128)
    wide = jnp.concatenate(
        [
            jnp.concatenate(
                [nf[pl.ds(t * 16 + h * 3 + i, 8, 32), :] for i in range(3)], axis=0
            )
            for t in range(2)
            for h in range(4)
        ],
        axis=1,
    ).astype(BF16)
    mixed = lax.dot_general(wide, wo[...], NT, preferred_element_type=F32)
    token_rows = [xs[pl.ds(pl.multiple_of(i * 16 + tp * 8, 8), 8), :] for i in range(3)]
    resid = (jnp.concatenate(token_rows, axis=0) + mixed).astype(BF16).astype(F32)
    res[...] = resid
    scaled2 = (resid * xs[49:50, :]).astype(BF16).astype(F32)
    total = lax.dot_general(
        jnp.ones((8, 128), F32),
        jnp.concatenate([resid * resid, jnp.zeros((104, 128), F32)], axis=0),
        NT,
        preferred_element_type=F32,
        precision=lax.Precision.HIGHEST,
    )
    total_hi = total.astype(BF16).astype(F32)
    r8 = iota((8, 128), 0)
    tail = jnp.where(r8 == 0, total_hi, jnp.where(r8 == 1, total - total_hi, 0.0))
    rsend[...] = jnp.concatenate([scaled2, tail], axis=0).astype(BF16)
    along(lambda far: rsend, rrecv.at[z], 6)
    rrecv[z] = rsend[...]
    for m, (a, b) in ((0, (15, 16)), (1, (17, 18))):
        got(fbuf.at[tp, y, m, ahead], fsem.at[a])
        got(fbuf.at[tp, y, m, behind], fsem.at[b])
        push(fbuf.at[tp, across, m], fbuf.at[tp, across, m], 7, sibling, fsem.at[12])
    got(rrecv.at[pl.ds(0, NZ - 1)], rsem.at[6])
    rows = jnp.concatenate([rrecv[k] for k in range(NZ)], axis=1)
    sums = rrecv[0, 16:32, :].astype(F32)
    for k in range(1, NZ):
        sums = sums + rrecv[k, 16:32, :].astype(F32)
    squares = sums[8:9] + sums[9:10]
    scale = lax.rsqrt(squares / D + 1e-06)
    dr, dc = iota((32, 128), 0), iota((32, 128), 1)
    scale = jnp.sum(jnp.where(dr == dc, scale, 0.0), axis=1, keepdims=True)
    got(fbuf.at[0], fsem.at[12])
    up_w = fbuf[:, :, 0].reshape(512, D)
    up = lax.dot_general(rows, up_w, NT, preferred_element_type=F32) * scale
    act = jnp.square(jnp.maximum(up, 0.0)).astype(BF16)
    for group in ((8, 7, 9, 6), (10, 5, 11, 4), (12, 3, 13, 2), (14, 1, 15, 0)):
        away = [(z + d) % NZ for d in group]
        down_w = jnp.concatenate(
            [
                fbuf[:, :, 1, :, pl.ds(pl.multiple_of(far * 128, 128), 128)].reshape(512, 128)
                for far in away
            ],
            axis=1,
        )
        part = jnp.dot(act, down_w, preferred_element_type=F32).astype(BF16)
        for n, (d, far) in enumerate(zip(group, away)):
            dsend[far] = part[:24, n * 128 : (n + 1) * 128]
            if d:
                push(dsend.at[far], drecv.at[z], 13, {"kv": far * NY + y})
    drecv[z] = dsend[z]
    got(drecv.at[pl.ds(0, NZ - 1)], rsem.at[13])
    final = res[...]
    for k in range(NZ):
        final = final + drecv[k].astype(F32)
    final = jnp.concatenate([final, jnp.zeros((104, 128), F32)], axis=0).T
    ysend[...] = final.astype(BF16).reshape(8, 16, 128)
    to_eight(lambda p: ysend.at[p], yrecv.at[me8], 14)
    yrecv[me8] = ysend[me8]
    got(yrecv.at[pl.ds(0, 7)], rsem.at[14])
    pieces = jnp.concatenate([yrecv[k] for k in range(8)], axis=1)
    placed = jnp.dot(pieces, qbuf[...], preferred_element_type=F32)
    out_ref[...] = placed[:, :192].astype(BF16)

    got(tbuf.at[pl.ds(0, 7)], ssem.at[0])
    got(wbuf.at[pl.ds(0, 2)], ssem.at[1])
    got(wbuf.at[0], ssem.at[2])
    got(fbuf.at[tp, pl.ds(0, 2)], ssem.at[3])
    got(zsend.at[pl.ds(0, NZ - 1)], ssem.at[4])

    @pl.when(half == tp)
    def _():
        got(nrecv.at[pl.ds(0, 15)], ssem.at[5])

    @pl.when(half != tp)
    def _():
        got(nrecv, ssem.at[5])

    got(rrecv.at[pl.ds(0, NZ - 1)], ssem.at[6])
    got(fbuf.at[tp], ssem.at[7])
    got(fbuf.at[tp, y], ssem.at[9])
    got(wo.at[pl.ds(0, 96), pl.ds(0, 512)], ssem.at[11])
    got(my_lanes, ssem.at[12])
    got(dsend.at[pl.ds(0, NZ - 1)], ssem.at[13])
    got(ysend.at[pl.ds(0, 7)], ssem.at[14])


def local_step(
    tokens,
    state,
    mix_gain,
    w_query,
    w_key,
    w_value,
    w_beta,
    w_decay,
    decay_log,
    head_gain,
    w_out,
    ff_gain,
    w_up,
    w_down,
):
    anywhere = pl.BlockSpec(memory_space=pltpu.HBM)
    vmem = pl.BlockSpec(memory_space=pltpu.VMEM)
    out, new_state = pl.pallas_call(
        body,
        name="layer",
        out_shape=(
            pltpu.VMEM((16, 192), BF16),
            pltpu.VMEM(state.shape, F32),
        ),
        in_specs=[anywhere] * 14,
        out_specs=(vmem, vmem),
        scratch_shapes=[
            pltpu.VMEM((16, 192), BF16),
            pltpu.VMEM((1, 16), BF16),
            pltpu.VMEM((1, 16), BF16),
            pltpu.VMEM((4, 32), BF16),
            pltpu.VMEM((4, 32), BF16),
            pltpu.VMEM((1, 128), BF16),
            pltpu.VMEM((1, 4), F32),
            pltpu.VMEM((8, 16, 256), BF16),
            pltpu.VMEM((NY, 3, 32, 512), BF16),
            pltpu.VMEM((128, 1024), BF16),
            pltpu.VMEM((2, NY, 2, 64, D), BF16),
            pltpu.VMEM((3, 4, 128, 128), F32),
            pltpu.VMEM((1024, 256), BF16),
            pltpu.VMEM((1024, 128), BF16),
            pltpu.VMEM((56, 128), F32),
            pltpu.VMEM((NZ * R1, 128), F32),
            pltpu.VMEM((NZ, R1, 128), BF16),
            pltpu.VMEM((NZ, R1, 128), BF16),
            pltpu.VMEM((R1, 128), F32),
            pltpu.VMEM((24, 128), F32),
            pltpu.VMEM((16, 128), F32),
            pltpu.VMEM((16, 128), BF16),
            pltpu.VMEM((16, 16, 128), BF16),
            pltpu.VMEM((256, 128), F32),
            pltpu.VMEM((32, 128), BF16),
            pltpu.VMEM((NZ, 32, 128), BF16),
            pltpu.VMEM((24, 128), F32),
            pltpu.VMEM((NZ, 24, 128), BF16),
            pltpu.VMEM((NZ, 24, 128), BF16),
            pltpu.VMEM((8, 16, 128), BF16),
            pltpu.VMEM((8, 16, 128), BF16),
            pltpu.SemaphoreType.DMA((14,)),
            pltpu.SemaphoreType.DMA((15,)),
            pltpu.SemaphoreType.DMA((15,)),
            pltpu.SemaphoreType.DMA((19,)),
            pltpu.SemaphoreType.REGULAR,
            pltpu.SemaphoreType.REGULAR,
            pltpu.SemaphoreType.REGULAR,
        ],
        compiler_params=pltpu.CompilerParams(
            collective_id=0, has_side_effects=True, vmem_limit_bytes=VMEM
        ),
    )(
        tokens.T,
        mix_gain[None, :],
        ff_gain[None, :],
        w_beta.T,
        w_decay.T,
        head_gain[None, :],
        decay_log[None, :],
        state,
        w_query,
        w_key,
        w_value,
        w_out.T,
        w_up.T,
        w_down,
    )
    return out.T, new_state


def solution(mesh):
    placed = (
        P("dp", ("kv", "tp")),
        P(("dp", "kv"), "tp", None, None),
        P(("kv", "tp")),
        P("kv", "tp"),
        P("kv", "tp"),
        P("kv", "tp"),
        P("kv", "tp"),
        P("kv", "tp"),
        P("tp"),
        P(),
        P("tp", "kv"),
        P(("kv", "tp")),
        P(None, ("kv", "tp")),
        P(("kv", "tp"), None),
    )
    return jax.shard_map(
        local_step,
        mesh=mesh,
        in_specs=placed,
        out_specs=(P("dp", ("kv", "tp")), P(("dp", "kv"), "tp", None, None)),
        check_vma=False,
    )
```

```python
import functools

import jax
import jax.numpy as jnp
from jax import lax
from jax.experimental import pallas as pl
from jax.experimental.pallas import tpu as pltpu
from jax.sharding import PartitionSpec as P

D = 2048
NZ = 16
NY = 4
MESH = pl.DeviceIdType.MESH
F32 = jnp.float32
BF16 = jnp.bfloat16
NT = (((1,), (1,)), ((), ()))
R1 = 40
GATE_AT = 200
VMEM = 60 * 1024 * 1024


def iota(shape, dim):
    return lax.broadcasted_iota(jnp.int32, shape, dim)


def body(
    tokens_hbm,
    mix_gain_hbm,
    ff_gain_hbm,
    beta_hbm,
    decay_hbm,
    head_gain_hbm,
    decay_log_hbm,
    state_hbm,
    wq_hbm,
    wk_hbm,
    wv_hbm,
    wo_hbm,
    wu_hbm,
    wd_hbm,
    out_ref,
    state_out,
    tok,
    mixg,
    ffg,
    bta,
    dcy,
    hgain,
    dlog,
    tbuf,
    wbuf,
    wo,
    fbuf,
    st,
    qbuf,
    ebuf,
    xs,
    zs,
    zsend,
    zrecv,
    accs,
    g12,
    hs,
    nsend,
    nrecv,
    nf,
    rsend,
    rrecv,
    res,
    dsend,
    drecv,
    ysend,
    yrecv,
    lsem,
    ssem,
    rsem,
    fsem,
    near_sem,
    mid_sem,
    far_sem,
):
    kv = lax.axis_index("kv")
    tp = lax.axis_index("tp")
    z = kv // NY
    y = kv % NY
    me8 = y * 2 + tp
    half = z // 8

    barrier = pltpu.get_barrier_semaphore()

    def local(src, dst, k):
        return pltpu.make_async_copy(src, dst, lsem.at[k])

    mine = wo.at[
        pl.ds(pl.multiple_of(y * 32, 32), 32), pl.ds(pl.multiple_of(tp * 512, 512), 512)
    ]

    loads = [
        local(wq_hbm, wbuf.at[y, 0], 5),
        local(wk_hbm, wbuf.at[y, 1], 6),
        local(wv_hbm, wbuf.at[y, 2], 7),
        local(tokens_hbm, tok, 0),
        local(mix_gain_hbm, mixg, 1),
        local(ff_gain_hbm, ffg, 2),
        local(beta_hbm, bta, 3),
        local(decay_hbm, dcy, 4),
        local(wo_hbm, mine, 8),
        local(wu_hbm, fbuf.at[tp, y, 0], 9),
        local(wd_hbm, fbuf.at[tp, y, 1], 10),
        local(head_gain_hbm, hgain, 11),
        local(decay_log_hbm, dlog, 12),
        local(state_hbm, st, 13),
    ]
    for c in loads[:3]:
        c.start()

    def greet(sem, where):
        pl.semaphore_signal(sem, inc=1, device_id=where, device_id_type=MESH)

    def on_ring(d):
        return {"kv": ((z + d) % NZ) * NY + y}

    def at_y(other):
        return {"kv": z * NY + other}

    above, below, across = (y + 1) % NY, (y + NY - 1) % NY, (y + 2) % NY
    sibling = {"tp": 1 - tp}
    beside = [at_y(above), at_y(below), on_ring(1), on_ring(NZ - 1)]
    diagonal = [{**at_y(above), **sibling}, {**at_y(below), **sibling}]
    for where in beside + [sibling] + diagonal:
        greet(barrier, where)
    for c in loads[3:8]:
        c.start()

    row, col = iota((56, 256), 0), iota((56, 256), 1)
    wanted = jnp.where(row < 48, 12 * (row % 16) + 3 * y + row // 16, row + 144)
    pick = jnp.where((col == wanted) & (row < 50), 1.0, 0.0).astype(BF16)

    pr, pc = iota((32, 256), 0), iota((32, 256), 1)
    shift = jnp.where(pc == pr + GATE_AT, 1.0, 0.0).astype(BF16)

    for c in loads[3:8]:
        c.wait()
    sr, sc = iota((16, 16), 0), iota((16, 16), 1)

    def upright(ref):
        return jnp.sum(jnp.where(sr == sc, ref[...].astype(F32), 0.0), axis=1, keepdims=True)

    gate_rows = jnp.concatenate([bta[...].astype(F32), dcy[...].astype(F32)], axis=0)
    gate_rows = jnp.concatenate([gate_rows, jnp.zeros((8, 32), F32)], axis=0).astype(BF16)
    lanes = iota((16, 256), 1)
    tile = jnp.dot(gate_rows, shift, preferred_element_type=F32)
    tile = jnp.where(lanes == 192, upright(mixg), jnp.where(lanes == 193, upright(ffg), tile))
    tile = tile + jnp.concatenate([tok[...].astype(F32), jnp.zeros((16, 64), F32)], axis=1)
    tbuf[me8] = tile.astype(BF16)
    for c in loads[:3]:
        c.wait()
    for c in loads[8:]:
        c.start()

    pl.semaphore_wait(barrier, 7)

    def push(src, dst, k, where, to=None):
        pltpu.make_async_remote_copy(
            src_ref=src,
            dst_ref=dst,
            send_sem=ssem.at[k],
            recv_sem=rsem.at[k] if to is None else to,
            device_id=where,
            device_id_type=MESH,
        ).start()

    def to_eight(src_of, dst, k):
        def one(j, carry):
            p = (me8 + j) % 8
            push(src_of(p), dst, k, {"kv": z * NY + p // 2, "tp": p % 2})
            return carry

        lax.fori_loop(1, 8, one, 0)

    def got(ref, sem):
        pltpu.make_async_copy(ref, ref, sem).wait()

    shown = tbuf.at[me8]
    for where in [at_y(above), at_y(below)] + diagonal + [sibling]:
        push(shown, shown, 0, where)
    high, low = pl.ds(0, 16), pl.ds(16, 16)

    def weights(part, where, k):
        push(wbuf.at[y, :, part], wbuf.at[y, :, part], 1, where, fsem.at[k])

    weights(high, at_y(above), 0)
    weights(low, at_y(below), 2)
    for where in beside:
        greet(near_sem, where)
    pl.semaphore_wait(near_sem, 4)
    push(shown, shown, 0, at_y(across))
    push(shown, shown, 0, {**at_y(across), **sibling})
    weights(low, at_y(above), 1)
    weights(high, at_y(below), 3)
    greet(mid_sem, on_ring(2))
    greet(mid_sem, on_ring(NZ - 2))
    got(wbuf.at[y, :, high], fsem.at[0])
    push(wbuf.at[below, :, high], wbuf.at[below, :, high], 2, at_y(above), fsem.at[4])
    got(wbuf.at[y, :, low], fsem.at[2])
    push(wbuf.at[above, :, low], wbuf.at[above, :, low], 2, at_y(below), fsem.at[5])
    pl.semaphore_wait(mid_sem, 2)
    greet(far_sem, on_ring(4))
    greet(far_sem, on_ring(NZ - 4))
    for c in loads[8:11]:
        c.wait()
    for other in (above, below, across):
        push(mine, mine, 11, at_y(other), fsem.at[8])
    for m, (a, b) in ((0, (6, 7)), (1, (10, 11))):
        push(fbuf.at[tp, y, m], fbuf.at[tp, y, m], 3, at_y(above), fsem.at[a])
        push(fbuf.at[tp, y, m], fbuf.at[tp, y, m], 3, at_y(below), fsem.at[b])
    push(fbuf.at[tp, y], fbuf.at[tp, y], 7, sibling, fsem.at[12])
    er, ec = iota((1024, 128), 0), iota((1024, 128), 1)
    into = er % 256 - GATE_AT
    spread = jnp.where((ec == er // 256 * 32 + into) & (into >= 0) & (into < 32), 1.0, 0.0)
    ebuf[...] = spread.astype(BF16)
    got(tbuf.at[pl.ds(0, 7)], rsem.at[0])
    tiles = tbuf[...]
    turned = tiles.reshape(128, 256)
    chosen = lax.dot_general(pick, turned, NT, preferred_element_type=F32)
    xs[...] = chosen
    x = chosen[:48]
    scaled = (x * chosen[48:49]).astype(BF16)
    square = jnp.sum(x * x, axis=1, keepdims=True)
    square_hi = square.astype(BF16).astype(F32)
    own = jnp.concatenate([tbuf[2 * k + tp] for k in range(NY)], axis=1)
    gate_w = jnp.dot(own, ebuf[...], preferred_element_type=F32)
    gate_w = jnp.where(iota((16, 128), 0) < 8, gate_w, 0.0).astype(BF16)
    gate_w = jnp.concatenate([gate_w, jnp.zeros((112, 128), BF16)], axis=0)
    gate = lax.dot_general(scaled, gate_w, NT, preferred_element_type=F32)
    gl = iota((48, 128), 1)
    gate = jnp.where(gl == 8, square_hi, jnp.where(gl == 9, square - square_hi, gate))

    got(wbuf.at[y, :, low], fsem.at[1])
    got(wbuf.at[y, :, high], fsem.at[3])
    got(wbuf.at[y, :, high], fsem.at[4])
    got(wbuf.at[y, :, low], fsem.at[5])
    for m in range(3):
        weight = wbuf[:, m].reshape(128, 512)
        part = jnp.dot(scaled, weight, preferred_element_type=F32)
        for h in range(4):
            for i in range(3):
                zs[pl.ds(m * 12 + h * 3 + i, NZ, R1), :] = part[
                    i * 16 : (i + 1) * 16, h * 128 : (h + 1) * 128
                ]
    for i in range(3):
        zs[pl.ds(36 + i, NZ, R1), :] = gate[i * 16 : (i + 1) * 16]
    zs[pl.ds(39, NZ, R1), :] = jnp.broadcast_to(chosen[49:50], (NZ, 128))
    zsend[...] = zs[...].reshape(NZ, R1, 128).astype(BF16)

    def along(src_of, dst, k, lower=0, upper=NZ - 1):
        def one(n, carry):
            d = NZ // 2 + ((n + 1) // 2) * (1 - 2 * (n % 2))
            far = (z + d) % NZ
            push(src_of(far), dst, k, {"kv": far * NY + y})
            return carry

        lax.fori_loop(lower, upper, one, 0)

    pl.semaphore_wait(far_sem, 2)
    along(lambda far: zsend.at[far], zrecv.at[z], 4)
    zrecv[z] = zsend[z]
    for c in loads[11:]:
        c.wait()
    src_row, seq_col = iota((1024, 256), 0), iota((1024, 256), 1)
    lane = src_row % 128
    place = 12 * ((src_row // 128 % 2) * 8 + lane % 8) + 3 * (src_row // 256) + lane // 8
    qbuf[...] = jnp.where((seq_col == place) & (lane < 24), 1.0, 0.0).astype(BF16)
    got(zrecv.at[pl.ds(0, NZ - 1)], rsem.at[4])

    acc = zrecv[0].astype(F32)
    for k in range(1, NZ):
        acc = acc + zrecv[k].astype(F32)
    accs[...] = acc
    for h in range(4):
        g12[3 * h : 3 * h + 3, :] = accs[36:39, :]
    g = g12[0:12, :]
    r12, l12 = iota((12, 128), 0), iota((12, 128), 1)
    head_of = r12 // 3

    def take(mask):
        return jnp.sum(jnp.where(mask, g, 0.0), axis=1, keepdims=True)

    inverse = lax.rsqrt(take((l12 == 8) | (l12 == 9)) / D + 1e-06)
    beta = jax.nn.sigmoid(inverse * take(l12 == head_of))
    u = inverse * take(l12 == head_of + 4)
    soft = jnp.maximum(u, 0.0) + jnp.log1p(jnp.exp(-jnp.abs(u)))
    lr, lc = iota((12, 4), 0), iota((12, 4), 1)
    rate = jnp.sum(jnp.where(lc == lr // 3, dlog[...], 0.0), axis=1, keepdims=True)
    keep = jnp.exp(-jnp.exp(rate) * soft)
    query, key = accs[0:12, :], accs[12:24, :]
    value = inverse * accs[24:36, :]
    square_of = inverse * inverse
    qsum = jnp.sum(query * query, axis=1, keepdims=True)
    ksum = jnp.sum(key * key, axis=1, keepdims=True)
    qnorm = query * (inverse * lax.rsqrt(square_of * qsum + 1e-06))
    knorm = key * (inverse * lax.rsqrt(square_of * ksum + 1e-06))
    pad = jnp.zeros((104, 128), F32)
    g12[0:12, :] = qnorm
    g12[12:24, :] = knorm
    both = jnp.concatenate([g12[...], pad], axis=0).T
    for r in range(12):
        h, i = r // 3, r % 3
        kc = both[:, 12 + r : 13 + r]
        qc = both[:, r : r + 1]
        kept = st[i, h] * keep[r : r + 1, :]
        predicted = jnp.sum(kept * kc, axis=0, keepdims=True)
        change = beta[r : r + 1, :] * (value[r : r + 1, :] - predicted)
        new = kept + kc * change
        state_out[i, h] = new
        hs[r : r + 1, :] = jnp.sum(new * qc, axis=0, keepdims=True)
    heads = hs[...] / jnp.sqrt(jnp.float32(128))
    heads = jnp.where(iota((16, 128), 0) < 12, heads, 0.0)
    normed = (
        heads
        * lax.rsqrt(jnp.mean(heads * heads, axis=1, keepdims=True) + 1e-06)
        * hgain[...].astype(F32)
    )
    nsend[...] = normed.astype(BF16)

    slot = (z % 8) * 2 + tp

    def spread_heads(n, carry):
        d = (NZ // 2 + ((n + 1) // 2) * (1 - 2 * (n % 2))) % NZ
        far = (z + d) % NZ
        push(nsend, nrecv.at[slot], 5, {"kv": far * NY + y, "tp": half})
        return carry

    lax.fori_loop(0, NZ - 1, spread_heads, 0)

    @pl.when(half == tp)
    def _():
        nrecv[slot] = nsend[...]

    @pl.when(half != tp)
    def _():
        push(nsend, nrecv.at[slot], 5, {"tp": half})

    ahead, behind = pl.ds(0, 32), pl.ds(32, 32)
    got(wo.at[pl.ds(0, 96), pl.ds(0, 512)], fsem.at[8])
    my_lanes = wo.at[:, pl.ds(pl.multiple_of(tp * 512, 512), 512)]
    push(my_lanes, my_lanes, 12, sibling)
    for m, (a, b, c, d) in ((0, (6, 7, 15, 16)), (1, (10, 11, 17, 18))):
        got(fbuf.at[tp, y, m], fsem.at[a])
        push(
            fbuf.at[tp, below, m, ahead], fbuf.at[tp, below, m, ahead], 9, at_y(above), fsem.at[c]
        )
        got(fbuf.at[tp, y, m], fsem.at[b])
        push(
            fbuf.at[tp, above, m, behind],
            fbuf.at[tp, above, m, behind],
            9,
            at_y(below),
            fsem.at[d],
        )
        for other in (above, below):
            push(fbuf.at[tp, other, m], fbuf.at[tp, other, m], 7, sibling, fsem.at[12])
    @pl.when(half == tp)
    def _():
        got(nrecv.at[pl.ds(0, 15)], rsem.at[5])

    @pl.when(half != tp)
    def _():
        got(nrecv, rsem.at[5])

    got(my_lanes, rsem.at[12])
    nf[...] = nrecv[...].astype(F32).reshape(256, 128)
    wide = jnp.concatenate(
        [
            jnp.concatenate(
                [nf[pl.ds(t * 16 + h * 3 + i, 8, 32), :] for i in range(3)], axis=0
            )
            for t in range(2)
            for h in range(4)
        ],
        axis=1,
    ).astype(BF16)
    mixed = lax.dot_general(wide, wo[...], NT, preferred_element_type=F32)
    token_rows = [xs[pl.ds(pl.multiple_of(i * 16 + tp * 8, 8), 8), :] for i in range(3)]
    resid = (jnp.concatenate(token_rows, axis=0) + mixed).astype(BF16).astype(F32)
    res[...] = resid
    rsend[...] = resid.astype(BF16)
    along(lambda far: rsend, rrecv.at[z], 6, 0, 5)
    along(lambda far: rsend, rrecv.at[z], 15, 5, NZ - 1)
    rrecv[z] = rsend[...]
    for m, (a, b) in ((0, (15, 16)), (1, (17, 18))):
        got(fbuf.at[tp, y, m, ahead], fsem.at[a])
        got(fbuf.at[tp, y, m, behind], fsem.at[b])
        push(fbuf.at[tp, across, m], fbuf.at[tp, across, m], 7, sibling, fsem.at[12])
    def entered(ds):
        parts, weights_of, spent = [], [], jnp.zeros((24, 128), F32)
        for d in ds:
            k = (z + d) % NZ
            part = rrecv[k].astype(F32)
            gain = zrecv[k, 32:40, :].astype(F32)[7:8]
            parts.append((part * gain).astype(BF16))
            spent = spent + part * part
            at = pl.multiple_of(k * 128, 128)
            weights_of.append(fbuf[:, :, 0, :, pl.ds(at, 128)].reshape(512, 128))
        up = lax.dot_general(
            jnp.concatenate(parts, axis=1),
            jnp.concatenate(weights_of, axis=1),
            NT,
            preferred_element_type=F32,
        )
        return up, spent

    got(rrecv.at[pl.ds(0, 10)], rsem.at[15])
    got(fbuf.at[0], fsem.at[12])
    up_near, spent_near = entered((0, 1, 15, 2, 14, 3, 13, 4, 12, 5, 11))
    got(rrecv.at[pl.ds(0, 5)], rsem.at[6])
    up_far, spent_far = entered((6, 10, 7, 9, 8))
    mean = jnp.sum(spent_near + spent_far, axis=1, keepdims=True) / D
    up = (up_near + up_far) * lax.rsqrt(mean + 1e-06)
    act = jnp.square(jnp.maximum(up, 0.0)).astype(BF16)
    for group in ((8, 7, 9, 6), (10, 5, 11, 4), (12, 3, 13, 2), (14, 1, 15, 0)):
        away = [(z + d) % NZ for d in group]
        down_w = jnp.concatenate(
            [
                fbuf[:, :, 1, :, pl.ds(pl.multiple_of(far * 128, 128), 128)].reshape(512, 128)
                for far in away
            ],
            axis=1,
        )
        part = jnp.dot(act, down_w, preferred_element_type=F32).astype(BF16)
        for n, (d, far) in enumerate(zip(group, away)):
            dsend[far] = part[:, n * 128 : (n + 1) * 128]
            if d:
                push(dsend.at[far], drecv.at[z], 13, {"kv": far * NY + y})
    drecv[z] = dsend[z]
    got(drecv.at[pl.ds(0, NZ - 1)], rsem.at[13])
    final = res[...]
    for k in range(NZ):
        final = final + drecv[k].astype(F32)
    final = jnp.concatenate([final, jnp.zeros((104, 128), F32)], axis=0).T
    ysend[...] = final.astype(BF16).reshape(8, 16, 128)
    to_eight(lambda p: ysend.at[p], yrecv.at[me8], 14)
    yrecv[me8] = ysend[me8]
    got(yrecv.at[pl.ds(0, 7)], rsem.at[14])
    pieces = jnp.concatenate([yrecv[k] for k in range(8)], axis=1)
    placed = jnp.dot(pieces, qbuf[...], preferred_element_type=F32)
    out_ref[...] = placed[:, :192].astype(BF16)

    got(tbuf.at[pl.ds(0, 7)], ssem.at[0])
    got(wbuf.at[pl.ds(0, 2)], ssem.at[1])
    got(wbuf.at[0], ssem.at[2])
    got(fbuf.at[tp, pl.ds(0, 2)], ssem.at[3])
    got(zsend.at[pl.ds(0, NZ - 1)], ssem.at[4])

    @pl.when(half == tp)
    def _():
        got(nrecv.at[pl.ds(0, 15)], ssem.at[5])

    @pl.when(half != tp)
    def _():
        got(nrecv, ssem.at[5])

    got(rrecv.at[pl.ds(0, 5)], ssem.at[6])
    got(rrecv.at[pl.ds(0, 10)], ssem.at[15])
    got(fbuf.at[tp], ssem.at[7])
    got(fbuf.at[tp, y], ssem.at[9])
    got(wo.at[pl.ds(0, 96), pl.ds(0, 512)], ssem.at[11])
    got(my_lanes, ssem.at[12])
    got(dsend.at[pl.ds(0, NZ - 1)], ssem.at[13])
    got(ysend.at[pl.ds(0, 7)], ssem.at[14])


def local_step(
    tokens,
    state,
    mix_gain,
    w_query,
    w_key,
    w_value,
    w_beta,
    w_decay,
    decay_log,
    head_gain,
    w_out,
    ff_gain,
    w_up,
    w_down,
):
    anywhere = pl.BlockSpec(memory_space=pltpu.HBM)
    vmem = pl.BlockSpec(memory_space=pltpu.VMEM)
    out, new_state = pl.pallas_call(
        body,
        name="layer",
        out_shape=(
            pltpu.VMEM((16, 192), BF16),
            pltpu.VMEM(state.shape, F32),
        ),
        in_specs=[anywhere] * 14,
        out_specs=(vmem, vmem),
        scratch_shapes=[
            pltpu.VMEM((16, 192), BF16),
            pltpu.VMEM((1, 16), BF16),
            pltpu.VMEM((1, 16), BF16),
            pltpu.VMEM((4, 32), BF16),
            pltpu.VMEM((4, 32), BF16),
            pltpu.VMEM((1, 128), BF16),
            pltpu.VMEM((1, 4), F32),
            pltpu.VMEM((8, 16, 256), BF16),
            pltpu.VMEM((NY, 3, 32, 512), BF16),
            pltpu.VMEM((128, 1024), BF16),
            pltpu.VMEM((2, NY, 2, 64, D), BF16),
            pltpu.VMEM((3, 4, 128, 128), F32),
            pltpu.VMEM((1024, 256), BF16),
            pltpu.VMEM((1024, 128), BF16),
            pltpu.VMEM((56, 128), F32),
            pltpu.VMEM((NZ * R1, 128), F32),
            pltpu.VMEM((NZ, R1, 128), BF16),
            pltpu.VMEM((NZ, R1, 128), BF16),
            pltpu.VMEM((R1, 128), F32),
            pltpu.VMEM((24, 128), F32),
            pltpu.VMEM((16, 128), F32),
            pltpu.VMEM((16, 128), BF16),
            pltpu.VMEM((16, 16, 128), BF16),
            pltpu.VMEM((256, 128), F32),
            pltpu.VMEM((24, 128), BF16),
            pltpu.VMEM((NZ, 24, 128), BF16),
            pltpu.VMEM((24, 128), F32),
            pltpu.VMEM((NZ, 24, 128), BF16),
            pltpu.VMEM((NZ, 24, 128), BF16),
            pltpu.VMEM((8, 16, 128), BF16),
            pltpu.VMEM((8, 16, 128), BF16),
            pltpu.SemaphoreType.DMA((14,)),
            pltpu.SemaphoreType.DMA((16,)),
            pltpu.SemaphoreType.DMA((16,)),
            pltpu.SemaphoreType.DMA((19,)),
            pltpu.SemaphoreType.REGULAR,
            pltpu.SemaphoreType.REGULAR,
            pltpu.SemaphoreType.REGULAR,
        ],
        compiler_params=pltpu.CompilerParams(
            collective_id=0, has_side_effects=True, vmem_limit_bytes=VMEM
        ),
    )(
        tokens.T,
        mix_gain[None, :],
        ff_gain[None, :],
        w_beta.T,
        w_decay.T,
        head_gain[None, :],
        decay_log[None, :],
        state,
        w_query,
        w_key,
        w_value,
        w_out.T,
        w_up.T,
        w_down,
    )
    return out.T, new_state


def solution(mesh):
    placed = (
        P("dp", ("kv", "tp")),
        P(("dp", "kv"), "tp", None, None),
        P(("kv", "tp")),
        P("kv", "tp"),
        P("kv", "tp"),
        P("kv", "tp"),
        P("kv", "tp"),
        P("kv", "tp"),
        P("tp"),
        P(),
        P("tp", "kv"),
        P(("kv", "tp")),
        P(None, ("kv", "tp")),
        P(("kv", "tp"), None),
    )
    return jax.shard_map(
        local_step,
        mesh=mesh,
        in_specs=placed,
        out_specs=(P("dp", ("kv", "tp")), P(("dp", "kv"), "tp", None, None)),
        check_vma=False,
    )
```

```python
import functools

import jax
import jax.numpy as jnp
from jax import lax
from jax.experimental import pallas as pl
from jax.experimental.pallas import tpu as pltpu
from jax.sharding import PartitionSpec as P

D = 2048
NZ = 16
NY = 4
MESH = pl.DeviceIdType.MESH
F32 = jnp.float32
BF16 = jnp.bfloat16
NT = (((1,), (1,)), ((), ()))
GATE_AT = 200
VMEM = 60 * 1024 * 1024


def iota(shape, dim):
    return lax.broadcasted_iota(jnp.int32, shape, dim)


def body(
    tokens_hbm,
    mix_gain_hbm,
    ff_gain_hbm,
    beta_hbm,
    decay_hbm,
    head_gain_hbm,
    decay_log_hbm,
    state_hbm,
    wq_hbm,
    wk_hbm,
    wv_hbm,
    wo_hbm,
    wu_hbm,
    wd_hbm,
    out_ref,
    state_out,
    tok,
    mixg,
    ffg,
    bta,
    dcy,
    hgain,
    dlog,
    tbuf,
    wbuf,
    wo,
    fbuf,
    st,
    qbuf,
    ebuf,
    xs,
    za,
    asend,
    arecv,
    zs,
    zsend,
    zrecv,
    accs,
    keys,
    kt,
    us,
    gates_of,
    upn,
    spn,
    g12,
    hs,
    nsend,
    nrecv,
    nf,
    rsend,
    rrecv,
    res,
    dsend,
    drecv,
    ysend,
    yrecv,
    lsem,
    ssem,
    rsem,
    fsem,
    near_sem,
    mid_sem,
    far_sem,
):
    kv = lax.axis_index("kv")
    tp = lax.axis_index("tp")
    z = kv // NY
    y = kv % NY
    me8 = y * 2 + tp
    half = z // 8

    barrier = pltpu.get_barrier_semaphore()

    def local(src, dst, k):
        return pltpu.make_async_copy(src, dst, lsem.at[k])

    mine = wo.at[
        pl.ds(pl.multiple_of(y * 32, 32), 32), pl.ds(pl.multiple_of(tp * 512, 512), 512)
    ]

    loads = [
        local(wq_hbm, wbuf.at[y, 0], 5),
        local(wk_hbm, wbuf.at[y, 1], 6),
        local(wv_hbm, wbuf.at[y, 2], 7),
        local(tokens_hbm, tok, 0),
        local(mix_gain_hbm, mixg, 1),
        local(ff_gain_hbm, ffg, 2),
        local(beta_hbm, bta, 3),
        local(decay_hbm, dcy, 4),
        local(wo_hbm, mine, 8),
        local(wu_hbm, fbuf.at[tp, y, 0], 9),
        local(wd_hbm, fbuf.at[tp, y, 1], 10),
        local(head_gain_hbm, hgain, 11),
        local(decay_log_hbm, dlog, 12),
        local(state_hbm, st, 13),
    ]
    for c in loads[:3]:
        c.start()

    def greet(sem, where):
        pl.semaphore_signal(sem, inc=1, device_id=where, device_id_type=MESH)

    def on_ring(d):
        return {"kv": ((z + d) % NZ) * NY + y}

    def at_y(other):
        return {"kv": z * NY + other}

    above, below, across = (y + 1) % NY, (y + NY - 1) % NY, (y + 2) % NY
    sibling = {"tp": 1 - tp}
    beside = [at_y(above), at_y(below), on_ring(1), on_ring(NZ - 1)]
    diagonal = [{**at_y(above), **sibling}, {**at_y(below), **sibling}]
    for where in beside + [sibling] + diagonal:
        greet(barrier, where)
    for c in loads[3:8]:
        c.start()

    for c in loads[:3]:
        c.wait()
    for c in loads[8:]:
        c.start()

    pl.semaphore_wait(barrier, 7)

    def push(src, dst, k, where, to=None):
        pltpu.make_async_remote_copy(
            src_ref=src,
            dst_ref=dst,
            send_sem=ssem.at[k],
            recv_sem=rsem.at[k] if to is None else to,
            device_id=where,
            device_id_type=MESH,
        ).start()

    def to_eight(src_of, dst, k):
        def one(j, carry):
            p = (me8 + j) % 8
            push(src_of(p), dst, k, {"kv": z * NY + p // 2, "tp": p % 2})
            return carry

        lax.fori_loop(1, 8, one, 0)

    def got(ref, sem):
        pltpu.make_async_copy(ref, ref, sem).wait()

    high, low = pl.ds(0, 16), pl.ds(16, 16)

    asks, rest = pl.ds(0, 1), pl.ds(1, 2)

    def weights(cols, part, where, k):
        shard = wbuf.at[y, cols, part]
        push(shard, shard, 1, where, fsem.at[k])

    weights(asks, high, at_y(above), 0)
    weights(asks, low, at_y(below), 2)
    weights(asks, low, at_y(above), 1)
    weights(asks, high, at_y(below), 3)
    weights(rest, high, at_y(above), 13)
    weights(rest, low, at_y(below), 14)
    for where in beside:
        greet(near_sem, where)
    row, col = iota((56, 256), 0), iota((56, 256), 1)
    wanted = jnp.where(row < 48, 12 * (row % 16) + 3 * y + row // 16, row + 144)
    pick = jnp.where((col == wanted) & (row < 50), 1.0, 0.0).astype(BF16)

    pr, pc = iota((32, 256), 0), iota((32, 256), 1)
    shift = jnp.where(pc == pr + GATE_AT, 1.0, 0.0).astype(BF16)

    for c in loads[3:8]:
        c.wait()
    sr, sc = iota((16, 16), 0), iota((16, 16), 1)

    def upright(ref):
        return jnp.sum(jnp.where(sr == sc, ref[...].astype(F32), 0.0), axis=1, keepdims=True)

    gate_rows = jnp.concatenate([bta[...].astype(F32), dcy[...].astype(F32)], axis=0)
    gate_rows = jnp.concatenate([gate_rows, jnp.zeros((8, 32), F32)], axis=0).astype(BF16)
    lanes = iota((16, 256), 1)
    tile = jnp.dot(gate_rows, shift, preferred_element_type=F32)
    tile = jnp.where(lanes == 192, upright(mixg), jnp.where(lanes == 193, upright(ffg), tile))
    tile = tile + jnp.concatenate([tok[...].astype(F32), jnp.zeros((16, 64), F32)], axis=1)
    tbuf[me8] = tile.astype(BF16)
    shown = tbuf.at[me8]
    for where in [at_y(above), at_y(below)] + diagonal + [sibling]:
        push(shown, shown, 0, where)
    pl.semaphore_wait(near_sem, 4)
    push(shown, shown, 0, at_y(across))
    push(shown, shown, 0, {**at_y(across), **sibling})
    weights(rest, low, at_y(above), 8)
    weights(rest, high, at_y(below), 9)
    greet(mid_sem, on_ring(2))
    greet(mid_sem, on_ring(NZ - 2))
    pl.semaphore_wait(mid_sem, 2)
    greet(far_sem, on_ring(4))
    greet(far_sem, on_ring(NZ - 4))
    for cols, (a, b, c, d) in ((asks, (0, 2, 4, 5)), (rest, (13, 14, 19, 20))):
        got(wbuf.at[y, cols, high], fsem.at[a])
        shard = wbuf.at[below, cols, high]
        push(shard, shard, 2, at_y(above), fsem.at[c])
        got(wbuf.at[y, cols, low], fsem.at[b])
        shard = wbuf.at[above, cols, low]
        push(shard, shard, 2, at_y(below), fsem.at[d])
    er, ec = iota((1024, 128), 0), iota((1024, 128), 1)
    into = er % 256 - GATE_AT
    spread = jnp.where((ec == er // 256 * 32 + into) & (into >= 0) & (into < 32), 1.0, 0.0)
    ebuf[...] = spread.astype(BF16)
    got(tbuf.at[pl.ds(0, 7)], rsem.at[0])
    tiles = tbuf[...]
    turned = tiles.reshape(128, 256)
    chosen = lax.dot_general(pick, turned, NT, preferred_element_type=F32)
    xs[...] = chosen
    x = chosen[:48]
    scaled = (x * chosen[48:49]).astype(BF16)
    square = jnp.sum(x * x, axis=1, keepdims=True)
    square_hi = square.astype(BF16).astype(F32)
    own = jnp.concatenate([tbuf[2 * k + tp] for k in range(NY)], axis=1)
    gate_w = jnp.dot(own, ebuf[...], preferred_element_type=F32)
    gate_w = jnp.where(iota((16, 128), 0) < 8, gate_w, 0.0).astype(BF16)
    gate_w = jnp.concatenate([gate_w, jnp.zeros((112, 128), BF16)], axis=0)
    gate = lax.dot_general(scaled, gate_w, NT, preferred_element_type=F32)
    gl = iota((48, 128), 1)
    gate = jnp.where(gl == 8, square_hi, jnp.where(gl == 9, square - square_hi, gate))


    def complete(cols, ks):
        for part, k in zip((low, high, high, low), ks):
            got(wbuf.at[y, cols, part], fsem.at[k])

    complete(asks, (1, 3, 4, 5))
    part = jnp.dot(scaled, wbuf[:, 0].reshape(128, 512), preferred_element_type=F32)
    for h in range(4):
        for i in range(3):
            za[pl.ds(h * 3 + i, NZ, 16), :] = part[
                i * 16 : (i + 1) * 16, h * 128 : (h + 1) * 128
            ]
    for i in range(3):
        za[pl.ds(12 + i, NZ, 16), :] = gate[i * 16 : (i + 1) * 16]
    za[pl.ds(15, NZ, 16), :] = jnp.broadcast_to(chosen[49:50], (NZ, 128))
    asend[...] = za[...].reshape(NZ, 16, 128).astype(BF16)

    def along(src_of, dst, k, lower=0, upper=NZ - 1):
        def one(n, carry):
            d = NZ // 2 + ((n + 1) // 2) * (1 - 2 * (n % 2))
            far = (z + d) % NZ
            push(src_of(far), dst, k, {"kv": far * NY + y})
            return carry

        lax.fori_loop(lower, upper, one, 0)

    pl.semaphore_wait(far_sem, 2)
    along(lambda far: asend.at[far], arecv.at[z], 4)
    complete(rest, (8, 9, 19, 20))
    for m in range(1, 3):
        part = jnp.dot(scaled, wbuf[:, m].reshape(128, 512), preferred_element_type=F32)
        for h in range(4):
            for i in range(3):
                zs[pl.ds((m - 1) * 12 + h * 3 + i, NZ, 24), :] = part[
                    i * 16 : (i + 1) * 16, h * 128 : (h + 1) * 128
                ]
    zsend[...] = zs[...].reshape(NZ, 24, 128).astype(BF16)
    along(lambda far: zsend.at[far], zrecv.at[z], 8)
    for c in loads[8:11]:
        c.wait()
    for other in (above, below, across):
        push(mine, mine, 11, at_y(other), rsem.at[2])
    for m, (a, b) in ((0, (6, 7)), (1, (10, 11))):
        push(fbuf.at[tp, y, m], fbuf.at[tp, y, m], 3, at_y(above), fsem.at[a])
        push(fbuf.at[tp, y, m], fbuf.at[tp, y, m], 3, at_y(below), fsem.at[b])
    push(fbuf.at[tp, y], fbuf.at[tp, y], 7, sibling, fsem.at[12])
    zrecv[z] = zsend[z]
    arecv[z] = asend[z]
    for c in loads[11:]:
        c.wait()
    src_row, seq_col = iota((1024, 256), 0), iota((1024, 256), 1)
    lane = src_row % 128
    place = 12 * ((src_row // 128 % 2) * 8 + lane % 8) + 3 * (src_row // 256) + lane // 8
    qbuf[...] = jnp.where((seq_col == place) & (lane < 24), 1.0, 0.0).astype(BF16)
    got(arecv.at[pl.ds(0, NZ - 1)], rsem.at[4])
    acc = arecv[0].astype(F32)
    for k in range(1, NZ):
        acc = acc + arecv[k].astype(F32)
    accs[0:16, :] = acc
    for h in range(4):
        g12[3 * h : 3 * h + 3, :] = accs[12:15, :]
    g = g12[0:12, :]
    r12, l12 = iota((12, 128), 0), iota((12, 128), 1)
    head_of = r12 // 3

    def take(mask):
        return jnp.sum(jnp.where(mask, g, 0.0), axis=1, keepdims=True)

    inverse = lax.rsqrt(take((l12 == 8) | (l12 == 9)) / D + 1e-06)
    beta = jax.nn.sigmoid(inverse * take(l12 == head_of))
    u = inverse * take(l12 == head_of + 4)
    soft = jnp.maximum(u, 0.0) + jnp.log1p(jnp.exp(-jnp.abs(u)))
    lr, lc = iota((12, 4), 0), iota((12, 4), 1)
    rate = jnp.sum(jnp.where(lc == lr // 3, dlog[...], 0.0), axis=1, keepdims=True)
    keep = jnp.exp(-jnp.exp(rate) * soft)
    square_of = inverse * inverse

    def unit(rows):
        size = jnp.sum(rows * rows, axis=1, keepdims=True)
        return rows * (inverse * lax.rsqrt(square_of * size + 1e-06))

    pad = jnp.zeros((112, 128), F32)
    qnorm = unit(accs[0:12, :])
    keys[0:12, :] = qnorm
    keys[12:16, :] = jnp.zeros((4, 128), F32)
    across_q = jnp.concatenate([keys[...], pad], axis=0).T
    for r in range(12):
        h, i = r // 3, r % 3
        kept = st[i, h] * keep[r : r + 1, :]
        st[i, h] = kept
        hs[r : r + 1, :] = jnp.sum(kept * across_q[:, r : r + 1], axis=0, keepdims=True)
    gates_of[:, 0:1] = beta
    gates_of[:, 1:2] = inverse
    gates_of[:, 2:3] = square_of
    got(zrecv.at[pl.ds(0, NZ - 1)], rsem.at[8])
    acc = zrecv[0].astype(F32)
    for k in range(1, NZ):
        acc = acc + zrecv[k].astype(F32)
    accs[16:40, :] = acc
    beta, inverse, square_of = gates_of[:, 0:1], gates_of[:, 1:2], gates_of[:, 2:3]
    knorm = unit(accs[16:28, :])
    value = inverse * accs[28:40, :]
    shared = jnp.sum(knorm * keys[0:12, :], axis=1, keepdims=True)
    keys[0:12, :] = knorm
    kt[...] = jnp.concatenate([keys[...], pad], axis=0).T
    for r in range(12):
        us[r : r + 1, :] = jnp.sum(st[r % 3, r // 3] * kt[:, r : r + 1], axis=0, keepdims=True)
    change = beta * (value - us[0:12, :])
    us[0:12, :] = change
    heads = (hs[0:12, :] + shared * change) / jnp.sqrt(jnp.float32(128))
    heads = jnp.concatenate([heads, jnp.zeros((4, 128), F32)], axis=0)
    normed = (
        heads
        * lax.rsqrt(jnp.mean(heads * heads, axis=1, keepdims=True) + 1e-06)
        * hgain[...].astype(F32)
    )
    nsend[...] = normed.astype(BF16)

    slot = (z % 8) * 2 + tp

    def spread_heads(n, carry):
        d = (NZ // 2 + ((n + 1) // 2) * (1 - 2 * (n % 2))) % NZ
        far = (z + d) % NZ
        push(nsend, nrecv.at[slot], 5, {"kv": far * NY + y, "tp": half})
        return carry

    lax.fori_loop(0, NZ - 1, spread_heads, 0)

    @pl.when(half == tp)
    def _():
        nrecv[slot] = nsend[...]

    @pl.when(half != tp)
    def _():
        push(nsend, nrecv.at[slot], 5, {"tp": half})

    for r in range(12):
        h, i = r // 3, r % 3
        state_out[i, h] = st[i, h] + kt[:, r : r + 1] * us[r : r + 1, :]
    ahead, behind = pl.ds(0, 32), pl.ds(32, 32)
    got(wo.at[pl.ds(0, 96), pl.ds(0, 512)], rsem.at[2])
    my_lanes = wo.at[:, pl.ds(pl.multiple_of(tp * 512, 512), 512)]
    push(my_lanes, my_lanes, 12, sibling)
    for m, (a, b, c, d) in ((0, (6, 7, 15, 16)), (1, (10, 11, 17, 18))):
        got(fbuf.at[tp, y, m], fsem.at[a])
        push(
            fbuf.at[tp, below, m, ahead], fbuf.at[tp, below, m, ahead], 9, at_y(above), fsem.at[c]
        )
        got(fbuf.at[tp, y, m], fsem.at[b])
        push(
            fbuf.at[tp, above, m, behind],
            fbuf.at[tp, above, m, behind],
            9,
            at_y(below),
            fsem.at[d],
        )
        for other in (above, below):
            push(fbuf.at[tp, other, m], fbuf.at[tp, other, m], 7, sibling, fsem.at[12])
    @pl.when(half == tp)
    def _():
        got(nrecv.at[pl.ds(0, 15)], rsem.at[5])

    @pl.when(half != tp)
    def _():
        got(nrecv, rsem.at[5])

    got(my_lanes, rsem.at[12])
    nf[...] = nrecv[...].astype(F32).reshape(256, 128)
    wide = jnp.concatenate(
        [
            jnp.concatenate(
                [nf[pl.ds(t * 16 + h * 3 + i, 8, 32), :] for i in range(3)], axis=0
            )
            for t in range(2)
            for h in range(4)
        ],
        axis=1,
    ).astype(BF16)
    mixed = lax.dot_general(wide, wo[...], NT, preferred_element_type=F32)
    token_rows = [xs[pl.ds(pl.multiple_of(i * 16 + tp * 8, 8), 8), :] for i in range(3)]
    resid = (jnp.concatenate(token_rows, axis=0) + mixed).astype(BF16).astype(F32)
    res[...] = resid
    rsend[...] = resid.astype(BF16)
    along(lambda far: rsend, rrecv.at[z], 6, 0, 3)
    along(lambda far: rsend, rrecv.at[z], 15, 3, NZ - 1)
    rrecv[z] = rsend[...]
    for m, (a, b) in ((0, (15, 16)), (1, (17, 18))):
        got(fbuf.at[tp, y, m, ahead], fsem.at[a])
        got(fbuf.at[tp, y, m, behind], fsem.at[b])
        push(fbuf.at[tp, across, m], fbuf.at[tp, across, m], 7, sibling, fsem.at[12])
    def entered(ds):
        parts, weights_of, spent = [], [], jnp.zeros((24, 128), F32)
        for d in ds:
            k = (z + d) % NZ
            part = rrecv[k].astype(F32)
            gain = arecv[k].astype(F32)[15:16]
            parts.append((part * gain).astype(BF16))
            spent = spent + part * part
            at = pl.multiple_of(k * 128, 128)
            weights_of.append(fbuf[:, :, 0, :, pl.ds(at, 128)].reshape(512, 128))
        up = lax.dot_general(
            jnp.concatenate(parts, axis=1),
            jnp.concatenate(weights_of, axis=1),
            NT,
            preferred_element_type=F32,
        )
        return up, spent

    got(rrecv.at[pl.ds(0, 12)], rsem.at[15])
    got(fbuf.at[0], fsem.at[12])
    up_near, spent_near = entered((0, 1, 15, 2, 14, 3, 13, 4, 12, 5, 11, 6, 10))
    upn[...] = up_near
    spn[...] = spent_near
    got(rrecv.at[pl.ds(0, 3)], rsem.at[6])
    up_far, spent_far = entered((7, 9, 8))
    mean = jnp.sum(spn[...] + spent_far, axis=1, keepdims=True) / D
    up = (upn[...] + up_far) * lax.rsqrt(mean + 1e-06)
    act = jnp.square(jnp.maximum(up, 0.0)).astype(BF16)
    for group in ((8, 7, 9, 6), (10, 5, 11, 4), (12, 3, 13, 2), (14, 1, 15, 0)):
        away = [(z + d) % NZ for d in group]
        down_w = jnp.concatenate(
            [
                fbuf[:, :, 1, :, pl.ds(pl.multiple_of(far * 128, 128), 128)].reshape(512, 128)
                for far in away
            ],
            axis=1,
        )
        part = jnp.dot(act, down_w, preferred_element_type=F32).astype(BF16)
        for n, (d, far) in enumerate(zip(group, away)):
            dsend[far] = part[:, n * 128 : (n + 1) * 128]
            if d:
                push(dsend.at[far], drecv.at[z], 13, {"kv": far * NY + y})
    drecv[z] = dsend[z]
    got(drecv.at[pl.ds(0, NZ - 1)], rsem.at[13])
    final = res[...]
    for k in range(NZ):
        final = final + drecv[k].astype(F32)
    final = jnp.concatenate([final, jnp.zeros((104, 128), F32)], axis=0).T
    ysend[...] = final.astype(BF16).reshape(8, 16, 128)
    to_eight(lambda p: ysend.at[p], yrecv.at[me8], 14)
    yrecv[me8] = ysend[me8]
    got(yrecv.at[pl.ds(0, 7)], rsem.at[14])
    pieces = jnp.concatenate([yrecv[k] for k in range(8)], axis=1)
    placed = jnp.dot(pieces, qbuf[...], preferred_element_type=F32)
    out_ref[...] = placed[:, :192].astype(BF16)

    got(tbuf.at[pl.ds(0, 7)], ssem.at[0])
    got(wbuf.at[pl.ds(0, 2)], ssem.at[1])
    got(wbuf.at[0], ssem.at[2])
    got(fbuf.at[tp, pl.ds(0, 2)], ssem.at[3])
    got(asend.at[pl.ds(0, NZ - 1)], ssem.at[4])
    got(zsend.at[pl.ds(0, NZ - 1)], ssem.at[8])

    @pl.when(half == tp)
    def _():
        got(nrecv.at[pl.ds(0, 15)], ssem.at[5])

    @pl.when(half != tp)
    def _():
        got(nrecv, ssem.at[5])

    got(rrecv.at[pl.ds(0, 3)], ssem.at[6])
    got(rrecv.at[pl.ds(0, 12)], ssem.at[15])
    got(fbuf.at[tp], ssem.at[7])
    got(fbuf.at[tp, y], ssem.at[9])
    got(wo.at[pl.ds(0, 96), pl.ds(0, 512)], ssem.at[11])
    got(my_lanes, ssem.at[12])
    got(dsend.at[pl.ds(0, NZ - 1)], ssem.at[13])
    got(ysend.at[pl.ds(0, 7)], ssem.at[14])


def leave(early_ref, state_ref, out_hbm, state_hbm, sem):
    copies = [
        pltpu.make_async_copy(state_ref, state_hbm, sem.at[0]),
        pltpu.make_async_copy(early_ref, out_hbm, sem.at[1]),
    ]
    for c in copies:
        c.start()
    for c in copies:
        c.wait()


def local_step(
    tokens,
    state,
    mix_gain,
    w_query,
    w_key,
    w_value,
    w_beta,
    w_decay,
    decay_log,
    head_gain,
    w_out,
    ff_gain,
    w_up,
    w_down,
):
    anywhere = pl.BlockSpec(memory_space=pltpu.HBM)
    vmem = pl.BlockSpec(memory_space=pltpu.VMEM)
    early, held = pl.pallas_call(
        body,
        name="layer",
        out_shape=(
            pltpu.VMEM((16, 192), BF16),
            pltpu.VMEM(state.shape, F32),
        ),
        in_specs=[anywhere] * 14,
        out_specs=(vmem, vmem),
        scratch_shapes=[
            pltpu.VMEM((16, 192), BF16),
            pltpu.VMEM((1, 16), BF16),
            pltpu.VMEM((1, 16), BF16),
            pltpu.VMEM((4, 32), BF16),
            pltpu.VMEM((4, 32), BF16),
            pltpu.VMEM((1, 128), BF16),
            pltpu.VMEM((1, 4), F32),
            pltpu.VMEM((8, 16, 256), BF16),
            pltpu.VMEM((NY, 3, 32, 512), BF16),
            pltpu.VMEM((128, 1024), BF16),
            pltpu.VMEM((2, NY, 2, 64, D), BF16),
            pltpu.VMEM((3, 4, 128, 128), F32),
            pltpu.VMEM((1024, 256), BF16),
            pltpu.VMEM((1024, 128), BF16),
            pltpu.VMEM((56, 128), F32),
            pltpu.VMEM((NZ * 16, 128), F32),
            pltpu.VMEM((NZ, 16, 128), BF16),
            pltpu.VMEM((NZ, 16, 128), BF16),
            pltpu.VMEM((NZ * 24, 128), F32),
            pltpu.VMEM((NZ, 24, 128), BF16),
            pltpu.VMEM((NZ, 24, 128), BF16),
            pltpu.VMEM((40, 128), F32),
            pltpu.VMEM((16, 128), F32),
            pltpu.VMEM((128, 128), F32),
            pltpu.VMEM((16, 128), F32),
            pltpu.VMEM((12, 128), F32),
            pltpu.VMEM((24, 512), F32),
            pltpu.VMEM((24, 128), F32),
            pltpu.VMEM((24, 128), F32),
            pltpu.VMEM((16, 128), F32),
            pltpu.VMEM((16, 128), BF16),
            pltpu.VMEM((16, 16, 128), BF16),
            pltpu.VMEM((256, 128), F32),
            pltpu.VMEM((24, 128), BF16),
            pltpu.VMEM((NZ, 24, 128), BF16),
            pltpu.VMEM((24, 128), F32),
            pltpu.VMEM((NZ, 24, 128), BF16),
            pltpu.VMEM((NZ, 24, 128), BF16),
            pltpu.VMEM((8, 16, 128), BF16),
            pltpu.VMEM((8, 16, 128), BF16),
            pltpu.SemaphoreType.DMA((14,)),
            pltpu.SemaphoreType.DMA((16,)),
            pltpu.SemaphoreType.DMA((16,)),
            pltpu.SemaphoreType.DMA((21,)),
            pltpu.SemaphoreType.REGULAR,
            pltpu.SemaphoreType.REGULAR,
            pltpu.SemaphoreType.REGULAR,
        ],
        compiler_params=pltpu.CompilerParams(
            collective_id=0, has_side_effects=True, vmem_limit_bytes=VMEM
        ),
    )(
        tokens.T,
        mix_gain[None, :],
        ff_gain[None, :],
        w_beta.T,
        w_decay.T,
        head_gain[None, :],
        decay_log[None, :],
        state,
        w_query,
        w_key,
        w_value,
        w_out.T,
        w_up.T,
        w_down,
    )
    out, new_state = pl.pallas_call(
        leave,
        name="leave",
        out_shape=(
            jax.ShapeDtypeStruct((16, 192), BF16),
            jax.ShapeDtypeStruct(state.shape, F32),
        ),
        in_specs=[pl.BlockSpec(memory_space=pl.ANY)] * 2,
        out_specs=(anywhere, anywhere),
        scratch_shapes=[pltpu.SemaphoreType.DMA((2,))],
        compiler_params=pltpu.CompilerParams(vmem_limit_bytes=1024 * 1024),
    )(early, held)
    return out.T, new_state


def solution(mesh):
    placed = (
        P("dp", ("kv", "tp")),
        P(("dp", "kv"), "tp", None, None),
        P(("kv", "tp")),
        P("kv", "tp"),
        P("kv", "tp"),
        P("kv", "tp"),
        P("kv", "tp"),
        P("kv", "tp"),
        P("tp"),
        P(),
        P("tp", "kv"),
        P(("kv", "tp")),
        P(None, ("kv", "tp")),
        P(("kv", "tp"), None),
    )
    return jax.shard_map(
        local_step,
        mesh=mesh,
        in_specs=placed,
        out_specs=(P("dp", ("kv", "tp")), P(("dp", "kv"), "tp", None, None)),
        check_vma=False,
    )
```
